768 devices in a mesh: ep: 48 (over z, x), tp: 16 (over y, core).
Axes of the slice: x: 4, y: 8, z: 12, core: 2. Of those that a mesh axis runs over, the one named last changes fastest.
Arguments:
- tokens: bfloat16 [12288, 4096], P('ep', 'tp'), may hold values from -540 to 540
- norm_gain: float32 [4096], P('tp'), may hold values from 0.1 to 1.9
- expert_ids: int32 [12288, 2], P('ep'), may hold values from 0 to 47, all different within a row; in each aligned block of 256 rows (0 to 255, 256 to 511, ...) at most 16 rows name the same one
- expert_weights: float32 [12288, 2], P('ep'), may hold values from 0.1 to 1
- gate_weight: bfloat16 [48, 4096, 2048], P('ep', None, 'tp'), may hold values from -0.09375 to 0.09375
- up_weight: bfloat16 [48, 4096, 2048], P('ep', None, 'tp'), may hold values from -0.09375 to 0.09375
- down_weight: bfloat16 [48, 2048, 4096], P('ep', None, 'tp'), may hold values from -0.125 to 0.125
Outputs:
- mixed: bfloat16 [12288, 4096], P('ep', 'tp')
The draws below stay inside these ranges and needn't reach their ends.
Inputs may be any that keep to these rules, and one draw needn't show every extreme that they name: `expert_ids`: each row names 2 different experts. Among the rows of one index of ep, no expert is named by more than 16 rows, a bound that some block reaches.
All inputs are finite; a program needn't handle non-finite values.
Results may differ from the reference program's by a relative error of at most 0.007.
Values may be sent and summed in bfloat16 or wider, within the bound.
No kernel may reach another device: no remote copies, remote signals or barrier semaphores. Data moves between devices by JAX's collectives and lax.ppermute only.
A program may use at most 64 MiB of HBM per device.

```python
import math
import jax
import jax.numpy as jnp
import numpy as np
from jax import lax

D = 4096
FF = 2048
TOPK = 2
TOK_DEV = 256
EXPERTS = 48
CAP = 16
TOKENS = 12288
N_EP = 48


def draw_tokens(key, part):
    key_base = jax.random.fold_in(key, 11)
    key_rows = jax.random.fold_in(key, 12)
    column = jnp.arange(D, dtype=jnp.float32) / D
    row_scale = jnp.exp(jax.random.uniform(key_rows, (TOKENS, 1), jnp.float32, 0.0, math.log(10.0)))
    base = jnp.clip(jax.random.normal(key_base, (TOKENS, D), jnp.float32), -6.0, 6.0)
    column_scale = 3.0 ** column
    return (base * column_scale[None, :] * row_scale).astype(jnp.bfloat16)


def steps_of(stream_key, dims, pieces, least, largest):
    level = 1.0
    for dim, shards_of in pieces:
        draws = jax.random.uniform(jax.random.fold_in(jax.random.fold_in(stream_key, 6), dim), (shards_of,), jnp.float32, least / len(pieces), largest / len(pieces))
        level = level * jnp.repeat(jnp.exp(draws), dims[dim] // shards_of).reshape((-1,) + (1,) * (len(dims) - 1 - dim))
    return level


def shared_out(key, own, number, rows, count, top, most, slope):
    sequence = jax.random.permutation(key, count)
    packed, usual = load_shares(count, rows * top, most, slope, True), load_shares(count, rows * top, most, slope, False)
    places = jnp.arange(count)

    def named(lengths, rotation):
        used = int((lengths > 0).sum())
        fixed = max(1, used // 4)
        shifted = fixed + (places - fixed + rotation * (used - fixed)) % max(1, count - fixed)
        return jnp.zeros((count,), jnp.int32).at[sequence[jnp.where(places < fixed, places, shifted)]].set(jnp.asarray(lengths, jnp.int32))

    lengths = jnp.where(number % 4 == 0, named(packed, number // 4), named(usual, number - number // 4 - 1))
    mixed = jax.random.permutation(jax.random.fold_in(own, 3), count)
    donor, taker = mixed[0:count // 2 * 2:2], mixed[1:count // 2 * 2:2]
    slack = jnp.minimum(lengths[donor] - 1, most - lengths[taker]) // 2
    slack = jnp.where((donor == sequence[0]) | (taker == sequence[0]) | (lengths[taker] == 0), 0, jnp.maximum(slack, 0))
    shifted = jax.random.randint(jax.random.fold_in(own, 4), (count // 2,), 0, 1 << 20) % (slack + 1)
    lengths = lengths.at[donor].add(-shifted).at[taker].add(shifted)
    labels = jnp.searchsorted(jnp.cumsum(lengths), jnp.arange(rows * top), side="right").astype(jnp.int32)
    listing = labels.reshape(top, rows).T
    listing = listing[jax.random.permutation(jax.random.fold_in(own, 1), rows)]
    rotation = jax.random.randint(jax.random.fold_in(own, 2), (rows, 1), 0, top)
    return jnp.take_along_axis(listing, (jnp.arange(top)[None, :] + rotation) % top, axis=1)


def load_shares(amount, total, limit, slope, full):
    loads = [(1 << 20) // math.isqrt(rank ** slope) + 1 for rank in range(1, amount + 1)]
    largest = limit if full else min(limit, max(-(-total // amount), total * loads[0] // sum(loads)))
    least = 1 if total - largest >= amount - 1 else 0
    counts, rest = [largest] + [least] * (amount - 1), total - largest - least * (amount - 1)
    while rest > 0:
        movable = [i for i in range(1, amount) if counts[i] < largest] or [i for i in range(1, amount) if counts[i] < limit]
        pool, budget = sum([loads[i] for i in movable]), rest
        for i in movable:
            addition = min(limit - counts[i], max(1, budget * loads[i] // pool), rest)
            counts[i] = counts[i] + addition
            rest = rest - addition
    return np.array(counts)


def bell_draw(rng, shape, width, bound, cuts=(), held_as=jnp.bfloat16):
    drawn = jax.random.normal(rng, shape, jnp.float32) * width
    if len(cuts) > 0:
        drawn = steps_of(rng, shape, cuts, -0.22, 0.18) * drawn
    return jnp.clip(drawn, min=-bound, max=bound).astype(held_as)


def setup_inputs(seed: int = 0) -> dict:
    keys = jax.random.split(jax.random.key(seed), 8)
    tokens = draw_tokens(jax.random.fold_in(keys[7], 71), 0)
    norm_gain = jnp.clip(1.0 + 0.18 * jax.random.normal(keys[1], (D,), jnp.float32), 0.1, 1.9)
    expert_ids_keys = jax.random.split(jax.random.fold_in(keys[2], 1), TOKENS // TOK_DEV)
    expert_ids_turns = jax.random.permutation(jax.random.fold_in(keys[2], 3), TOKENS // TOK_DEV)
    expert_ids = jax.vmap(lambda own, number: shared_out(jax.random.fold_in(keys[2], 2), own, number, TOK_DEV, EXPERTS, TOPK, CAP, 2))(expert_ids_keys, expert_ids_turns).reshape((TOKENS, TOPK))
    expert_weights = jnp.clip(0.1 + 0.9 * jax.random.uniform(keys[3], (TOKENS, TOPK), jnp.float32) ** steps_of(keys[3], (TOKENS, TOPK), ((0, 48),), -0.2, 0.2), 0.1, 1.0)
    gate_weight = bell_draw(keys[4], (EXPERTS, D, FF), D ** -0.5, 0.09375, ((0, 48), (2, 16)))
    up_weight = bell_draw(keys[5], (EXPERTS, D, FF), D ** -0.5, 0.09375, ((0, 48), (2, 16)))
    down_weight = bell_draw(keys[6], (EXPERTS, FF, D), FF ** -0.5, 0.125, ((0, 48), (2, 16)))
    return dict(tokens=tokens, norm_gain=norm_gain, expert_ids=expert_ids, expert_weights=expert_weights, gate_weight=gate_weight, up_weight=up_weight, down_weight=down_weight)


def reference(tokens, norm_gain, expert_ids, expert_weights, gate_weight, up_weight, down_weight):
    tok_f32 = tokens.astype(jnp.float32)
    inv_rms = lax.rsqrt(lax.optimization_barrier(jnp.mean(tok_f32 * tok_f32, axis=1, keepdims=True)) + 1e-06)
    normed = (tok_f32 * inv_rms * norm_gain[None, :]).astype(jnp.bfloat16)
    per_block = TOK_DEV * TOPK
    flat_ids = expert_ids.reshape(-1).astype(jnp.int32)
    blocked = flat_ids.reshape(N_EP, per_block)
    onehot = (blocked[:, :, None] == jnp.arange(EXPERTS, dtype=jnp.int32)[None, None, :]).astype(jnp.int32)
    earlier = jnp.cumsum(onehot, axis=1) - onehot
    slot_idx = lax.optimization_barrier(jnp.sum(earlier * onehot, axis=2)).reshape(-1).astype(jnp.int32)
    source = (jnp.arange(TOKENS * TOPK, dtype=jnp.int32) // per_block).astype(jnp.int32)
    position = (source * CAP + slot_idx).astype(jnp.int32)
    token_idx = (jnp.arange(TOKENS * TOPK, dtype=jnp.int32) // TOPK).astype(jnp.int32)
    buffers = jnp.zeros((EXPERTS, N_EP * CAP, D), jnp.bfloat16).at[flat_ids, position].set(normed[token_idx])

    def one_expert(operands):
        rows_in, w_gate, w_up, w_down = operands
        gate_sum = jnp.dot(rows_in, w_gate, preferred_element_type=jnp.float32)
        up_sum = jnp.dot(rows_in, w_up, preferred_element_type=jnp.float32)
        hidden = (jax.nn.silu(gate_sum) * up_sum).astype(jnp.bfloat16)
        return jnp.dot(hidden, w_down, preferred_element_type=jnp.float32).astype(jnp.bfloat16)
    results = lax.map(one_expert, (buffers, gate_weight, up_weight, down_weight))
    picked = results[flat_ids, position].astype(jnp.float32).reshape(TOKENS, TOPK, D)
    mixed = lax.optimization_barrier(jnp.sum(picked * expert_weights[:, :, None], axis=1))
    return mixed.astype(jnp.bfloat16)
```

```python
import functools

import jax
import jax.numpy as jnp
from jax import lax
from jax.experimental import pallas as pl
from jax.experimental.pallas import tpu as pltpu
from jax.sharding import Mesh, PartitionSpec as P

BF = jnp.bfloat16
F32 = jnp.float32
VM = pl.BlockSpec(memory_space=pltpu.VMEM)
SM = pl.BlockSpec(memory_space=pltpu.SMEM)
STEPS = (0, 1, -1, 2, -2, 3, -3, 4)
PAD = 8


def dot(a, b):
    return jnp.dot(a, b, preferred_element_type=F32)


def dispatch_kernel(experts, cap, ids_ref, tok_ref, out_ref, pick_ref):
    rows = tok_ref.shape[0]
    expert = lax.broadcasted_iota(jnp.int32, (experts, rows), 0)
    named = (expert == ids_ref[0:1, :]) | (expert == ids_ref[1:2, :])
    before = lax.broadcasted_iota(jnp.int32, (rows, rows), 0) < lax.broadcasted_iota(
        jnp.int32, (rows, rows), 1
    )
    rank = dot(named.astype(F32).astype(BF), before.astype(F32).astype(BF))
    rank = jnp.where(named, rank, -1.0)
    slot = lax.broadcasted_iota(jnp.int32, (cap, rows), 0).astype(F32)
    for e in range(experts):
        pick_ref[e * cap : (e + 1) * cap, :] = (
            (rank[e : e + 1, :] == slot).astype(F32).astype(BF)
        )
    out_ref[...] = dot(pick_ref[...], tok_ref[...]).astype(BF)


def combine_kernel(experts, cap, ids_ref, weight_ref, back_ref, out_ref):
    rows = out_ref.shape[0]
    line = lax.broadcasted_iota(jnp.int32, (8, rows), 0)
    table = jnp.where(line == 0, ids_ref[0:1, :].astype(F32), 0.0)
    table = jnp.where(line == 1, ids_ref[1:2, :].astype(F32), table)
    table = jnp.where(line == 2, weight_ref[0:1, :], table)
    table = jnp.where(line == 3, weight_ref[1:2, :], table)
    column = table.T
    first, second = column[:, 0:1], column[:, 1:2]
    lanes = lax.broadcasted_iota(jnp.int32, (rows, 128), 1).astype(F32)
    named = (lanes == first) | (lanes == second)
    after = lax.broadcasted_iota(jnp.int32, (rows, rows), 1) < lax.broadcasted_iota(
        jnp.int32, (rows, rows), 0
    )
    rank = dot(after.astype(F32).astype(BF), named.astype(F32).astype(BF))
    place = lax.broadcasted_iota(jnp.int32, (rows, experts * cap), 1).astype(F32)
    total = None
    for k, name in enumerate((first, second)):
        mine = jnp.sum(jnp.where(lanes == name, rank, 0.0), axis=1, keepdims=True)
        pick = (place == name * cap + mine).astype(F32).astype(BF)
        term = dot(pick, back_ref[...]) * column[:, 2 + k : 3 + k]
        total = term if total is None else total + term
    out_ref[...] = total.astype(BF)


def pack_kernel(where_ref, came_ref, gain_ref, peer_gain_ref, out_ref):
    sources = came_ref.shape[0] // 2
    width = came_ref.shape[2]
    for s in range(sources):
        for c in range(2):
            out_ref[s * 8 : s * 8 + 8, c * width : (c + 1) * width] = came_ref[2 * s + c]
    core = where_ref[1]
    mine, other = gain_ref[...], peer_gain_ref[...]
    gain = jnp.concatenate(
        [jnp.where(core == 0, mine, other), jnp.where(core == 0, other, mine)], axis=1
    )
    top = gain.astype(BF).astype(F32)
    mid = (gain - top).astype(BF).astype(F32)
    low = gain - top - mid
    line = lax.broadcasted_iota(jnp.int32, (PAD, 2 * width), 0)
    split = jnp.where(line == 0, top, jnp.where(line == 1, mid, jnp.where(line == 2, low, 0.0)))
    out_ref[sources * 8 : sources * 8 + PAD, :] = split.astype(BF)


def source_of(where_ref, step, count):
    turn = 1 - 2 * where_ref[1]
    return lax.rem(where_ref[0] - step * turn + 2 * count, count)


def hidden_kernel(count, where_ref, *refs):
    blocks, (gate_ref, gate2_ref, up_ref, up2_ref, out_ref, gsum, usum, square) = refs[:8], refs[8:]
    rows, half = out_ref.shape[0], gate_ref.shape[1]
    depth = blocks[0].shape[1]
    for number, (step, block) in enumerate(zip(STEPS, blocks)):
        start = pl.multiple_of(source_of(where_ref, step, count) * depth, depth)
        gain = jnp.sum(block[rows : rows + PAD, :].astype(F32), axis=0, keepdims=True)
        raw = block[0:rows, :].astype(F32)
        squares = raw * raw
        part = squares[:, 0:128]
        for lane in range(128, depth, 128):
            part = part + squares[:, lane : lane + 128]
        scaled = (raw * gain).astype(BF)
        gate = jnp.concatenate([gate_ref[pl.ds(start, depth), :], gate2_ref[pl.ds(start, depth), :]], axis=1)
        up = jnp.concatenate([up_ref[pl.ds(start, depth), :], up2_ref[pl.ds(start, depth), :]], axis=1)
        if number == 0:
            square[...] = part
            gsum[...] = dot(scaled, gate)
            usum[...] = dot(scaled, up)
        else:
            square[...] += part
            gsum[...] += dot(scaled, gate)
            usum[...] += dot(scaled, up)
    mean = jnp.sum(square[...], axis=1, keepdims=True) / (depth * count)
    scale = lax.rsqrt(mean + 1e-06)
    gate, up = gsum[...] * scale, usum[...] * scale
    hidden = (gate / (1.0 + jnp.exp(-gate)) * up).astype(BF)
    core = where_ref[1]
    out_ref[:, pl.ds(pl.multiple_of(core * half, half), half)] = hidden[:, :half]
    out_ref[:, pl.ds(pl.multiple_of((1 - core) * half, half), half)] = hidden[:, half:]


def down_kernel(count, where_ref, *refs):
    blocks, (down_ref, down2_ref, out_ref, mine, other) = refs[:8], refs[8:]
    depth = blocks[0].shape[1]
    for number, (step, block) in enumerate(zip(STEPS, blocks)):
        start = pl.multiple_of(source_of(where_ref, step, count) * depth, depth)
        first = dot(block[...], down_ref[pl.ds(start, depth), :])
        second = dot(block[...], down2_ref[pl.ds(start, depth), :])
        if number == 0:
            mine[...] = first
            other[...] = second
        else:
            mine[...] += first
            other[...] += second
    core = where_ref[1]
    for s in range(out_ref.shape[0]):
        out_ref[s, core] = mine[s * 8 : s * 8 + 8, :].astype(BF)
        out_ref[s, 1 - core] = other[s * 8 : s * 8 + 8, :].astype(BF)


def ring(block, count):
    def perm(sign):
        return [
            (y * 2 + c, (y + sign * (1 - 2 * c)) % count * 2 + c) for y in range(count) for c in range(2)
        ]

    main = other = block
    found = [block]
    for k in range(3):
        main = lax.ppermute(main, ("y", "c"), perm(1))
        other = lax.ppermute(other, ("y", "c"), perm(-1))
        found += [main, other]
    found.append(lax.ppermute(main, ("y", "c"), perm(1)))
    return found


def swap(value):
    return lax.ppermute(value, "c", [(0, 1), (1, 0)])


def body(tokens, norm_gain, expert_ids, expert_weights, gate_weight, up_weight, down_weight):
    count = lax.axis_size("y")
    experts = lax.axis_size("z") * lax.axis_size("x")
    rows, width = tokens.shape
    cap = 3 * rows * expert_ids.shape[1] // (2 * experts)
    half = experts * cap // 2
    where = jnp.stack([lax.axis_index("y"), lax.axis_index("c")]).astype(jnp.int32)
    ids = expert_ids.T
    call = functools.partial(pl.pallas_call)

    outgoing = call(
        functools.partial(dispatch_kernel, experts, cap),
        out_shape=jax.ShapeDtypeStruct((experts * cap, width), BF),
        in_specs=[VM, VM],
        out_specs=VM,
        scratch_shapes=[pltpu.VMEM((experts * cap, rows), BF)],
        name="dispatch",
    )(ids, tokens)
    came = lax.all_to_all(outgoing.reshape(2 * experts, 8, width), ("z", "x", "c"), 0, 0, tiled=True)

    gain = norm_gain[None, :]
    block = call(
        pack_kernel,
        out_shape=jax.ShapeDtypeStruct((half + PAD, 2 * width), BF),
        in_specs=[SM, VM, VM, VM],
        out_specs=VM,
        name="pack",
    )(where, came, gain, swap(gain))
    found = ring(block, count)

    gate, up, down = gate_weight[0], up_weight[0], down_weight[0]
    ff = gate.shape[1]
    hidden = call(
        functools.partial(hidden_kernel, count),
        out_shape=jax.ShapeDtypeStruct((half, 2 * ff), BF),
        in_specs=[SM] + [VM] * 12,
        out_specs=VM,
        scratch_shapes=[
            pltpu.VMEM((half, 2 * ff), F32),
            pltpu.VMEM((half, 2 * ff), F32),
            pltpu.VMEM((half, 128), F32),
        ],
        compiler_params=pltpu.CompilerParams(vmem_limit_bytes=40 << 20),
        name="hidden",
    )(where, *found, gate, swap(gate), up, swap(up))
    found = ring(hidden, count)

    made = call(
        functools.partial(down_kernel, count),
        out_shape=jax.ShapeDtypeStruct((experts, 2, 8, width), BF),
        in_specs=[SM] + [VM] * 10,
        out_specs=VM,
        scratch_shapes=[pltpu.VMEM((half, width), F32), pltpu.VMEM((half, width), F32)],
        compiler_params=pltpu.CompilerParams(vmem_limit_bytes=40 << 20),
        name="down",
    )(where, *found, down, swap(down))
    back = lax.all_to_all(made.reshape(2 * experts, 8, width), ("z", "x", "c"), 0, 0, tiled=True)

    return call(
        functools.partial(combine_kernel, experts, cap),
        out_shape=jax.ShapeDtypeStruct((rows, width), BF),
        in_specs=[VM, VM, VM],
        out_specs=VM,
        name="combine",
    )(ids, expert_weights.T, back.reshape(experts * cap, width))


def solution(mesh):
    split = Mesh(mesh.devices.reshape(12, 4, 8, 2), ("z", "x", "y", "c"))
    ep, tp = ("z", "x"), ("y", "c")
    in_specs = (
        P(ep, tp),
        P(tp),
        P(ep, None),
        P(ep, None),
        P(ep, None, tp),
        P(ep, None, tp),
        P(ep, None, tp),
    )
    return jax.shard_map(body, mesh=split, in_specs=in_specs, out_specs=P(ep, tp), check_vma=False)
```

```python
import functools

import jax
import jax.numpy as jnp
from jax import lax
from jax.experimental import pallas as pl
from jax.experimental.pallas import tpu as pltpu
from jax.sharding import Mesh, PartitionSpec as P

BF = jnp.bfloat16
F32 = jnp.float32
VM = pl.BlockSpec(memory_space=pltpu.VMEM)
SM = pl.BlockSpec(memory_space=pltpu.SMEM)
PAD = 8
CHUNKS = 2


def dot(a, b):
    return jnp.dot(a, b, preferred_element_type=F32)


def dispatch_kernel(experts, cap, ids_ref, tok_ref, out_ref, pick_ref):
    rows = tok_ref.shape[0]
    expert = lax.broadcasted_iota(jnp.int32, (experts, rows), 0)
    named = (expert == ids_ref[0:1, :]) | (expert == ids_ref[1:2, :])
    before = lax.broadcasted_iota(jnp.int32, (rows, rows), 0) < lax.broadcasted_iota(
        jnp.int32, (rows, rows), 1
    )
    rank = dot(named.astype(F32).astype(BF), before.astype(F32).astype(BF))
    rank = jnp.where(named, rank, -1.0)
    slot = lax.broadcasted_iota(jnp.int32, (cap, rows), 0).astype(F32)
    for e in range(experts):
        pick_ref[e * cap : (e + 1) * cap, :] = (
            (rank[e : e + 1, :] == slot).astype(F32).astype(BF)
        )
    out_ref[...] = dot(pick_ref[...], tok_ref[...]).astype(BF)


def combine_kernel(experts, cap, ids_ref, weight_ref, back_ref, out_ref):
    rows = out_ref.shape[0]
    line = lax.broadcasted_iota(jnp.int32, (8, rows), 0)
    table = jnp.where(line == 0, ids_ref[0:1, :].astype(F32), 0.0)
    table = jnp.where(line == 1, ids_ref[1:2, :].astype(F32), table)
    table = jnp.where(line == 2, weight_ref[0:1, :], table)
    table = jnp.where(line == 3, weight_ref[1:2, :], table)
    column = table.T
    first, second = column[:, 0:1], column[:, 1:2]
    lanes = lax.broadcasted_iota(jnp.int32, (rows, 128), 1).astype(F32)
    named = (lanes == first) | (lanes == second)
    after = lax.broadcasted_iota(jnp.int32, (rows, rows), 1) < lax.broadcasted_iota(
        jnp.int32, (rows, rows), 0
    )
    rank = dot(after.astype(F32).astype(BF), named.astype(F32).astype(BF))
    place = lax.broadcasted_iota(jnp.int32, (rows, experts * cap), 1).astype(F32)
    total = None
    for k, name in enumerate((first, second)):
        mine = jnp.sum(jnp.where(lanes == name, rank, 0.0), axis=1, keepdims=True)
        pick = (place == name * cap + mine).astype(F32).astype(BF)
        term = dot(pick, back_ref[...]) * column[:, 2 + k : 3 + k]
        total = term if total is None else total + term
    out_ref[...] = total.astype(BF)


def pack_kernel(where_ref, came_ref, gain_ref, peer_gain_ref, *out_refs):
    width = came_ref.shape[2]
    sources = came_ref.shape[0] // 2 // len(out_refs)
    core = where_ref[1]
    mine, other = gain_ref[...], peer_gain_ref[...]
    gain = jnp.concatenate(
        [jnp.where(core == 0, mine, other), jnp.where(core == 0, other, mine)], axis=1
    )
    top = gain.astype(BF).astype(F32)
    mid = (gain - top).astype(BF).astype(F32)
    low = gain - top - mid
    line = lax.broadcasted_iota(jnp.int32, (PAD, 2 * width), 0)
    split = jnp.where(line == 0, top, jnp.where(line == 1, mid, jnp.where(line == 2, low, 0.0)))
    for number, out_ref in enumerate(out_refs):
        for s in range(sources):
            for c in range(2):
                out_ref[s * 8 : s * 8 + 8, c * width : (c + 1) * width] = came_ref[
                    2 * (number * sources + s) + c
                ]
        out_ref[sources * 8 : sources * 8 + PAD, :] = split.astype(BF)


def source_of(where_ref, step, count):
    turn = 1 - 2 * where_ref[1]
    return lax.rem(where_ref[0] - step * turn + count, count)


def hidden_kernel(count, where_ref, *refs):
    blocks, (gate_ref, gate2_ref, up_ref, up2_ref, out_ref, gsum, usum, square) = refs[:count], refs[count:]
    rows, half = out_ref.shape[0], gate_ref.shape[1]
    depth = blocks[0].shape[1]
    for step, block in enumerate(blocks):
        start = pl.multiple_of(source_of(where_ref, step, count) * depth, depth)
        gain = jnp.sum(block[rows : rows + PAD, :].astype(F32), axis=0, keepdims=True)
        raw = block[0:rows, :].astype(F32)
        squares = raw * raw
        part = squares[:, 0:128]
        for lane in range(128, depth, 128):
            part = part + squares[:, lane : lane + 128]
        scaled = (raw * gain).astype(BF)
        gate = jnp.concatenate([gate_ref[pl.ds(start, depth), :], gate2_ref[pl.ds(start, depth), :]], axis=1)
        up = jnp.concatenate([up_ref[pl.ds(start, depth), :], up2_ref[pl.ds(start, depth), :]], axis=1)
        if step == 0:
            square[...] = part
            gsum[...] = dot(scaled, gate)
            usum[...] = dot(scaled, up)
        else:
            square[...] += part
            gsum[...] += dot(scaled, gate)
            usum[...] += dot(scaled, up)
    mean = jnp.sum(square[...], axis=1, keepdims=True) / (depth * count)
    scale = lax.rsqrt(mean + 1e-06)
    gate, up = gsum[...] * scale, usum[...] * scale
    hidden = (gate / (1.0 + jnp.exp(-gate)) * up).astype(BF)
    core = where_ref[1]
    out_ref[:, pl.ds(pl.multiple_of(core * half, half), half)] = hidden[:, :half]
    out_ref[:, pl.ds(pl.multiple_of((1 - core) * half, half), half)] = hidden[:, half:]


def down_kernel(count, where_ref, *refs):
    blocks, (down_ref, down2_ref, out_ref) = refs[: CHUNKS * count], refs[CHUNKS * count :]
    rows, depth = blocks[0].shape
    core = where_ref[1]
    for number in range(CHUNKS):
        mine = other = None
        for step, block in enumerate(blocks[number * count : (number + 1) * count]):
            start = pl.multiple_of(source_of(where_ref, step, count) * depth, depth)
            first = dot(block[...], down_ref[pl.ds(start, depth), :])
            second = dot(block[...], down2_ref[pl.ds(start, depth), :])
            mine = first if step == 0 else mine + first
            other = second if step == 0 else other + second
        for s in range(rows // 8):
            out_ref[number * rows // 8 + s, core] = mine[s * 8 : s * 8 + 8, :].astype(BF)
            out_ref[number * rows // 8 + s, 1 - core] = other[s * 8 : s * 8 + 8, :].astype(BF)


def ring(block, count):
    perm = [(y * 2 + c, (y + 1 - 2 * c) % count * 2 + c) for y in range(count) for c in range(2)]
    found = [block]
    for _ in range(count - 1):
        found.append(lax.ppermute(found[-1], ("y", "c"), perm))
    return found


def swap(value):
    return lax.ppermute(value, "c", [(0, 1), (1, 0)])


def body(tokens, norm_gain, expert_ids, expert_weights, gate_weight, up_weight, down_weight):
    count = lax.axis_size("y")
    experts = lax.axis_size("z") * lax.axis_size("x")
    rows, width = tokens.shape
    cap = 3 * rows * expert_ids.shape[1] // (2 * experts)
    half = experts * cap // 2
    where = jnp.stack([lax.axis_index("y"), lax.axis_index("c")]).astype(jnp.int32)
    ids = expert_ids.T
    call = pl.pallas_call

    outgoing = call(
        functools.partial(dispatch_kernel, experts, cap),
        out_shape=jax.ShapeDtypeStruct((experts * cap, width), BF),
        in_specs=[VM, VM],
        out_specs=VM,
        scratch_shapes=[pltpu.VMEM((experts * cap, rows), BF)],
        compiler_params=pltpu.CompilerParams(vmem_limit_bytes=8 << 20),
        name="dispatch",
    )(ids, tokens)
    came = lax.all_to_all(outgoing.reshape(2 * experts, 8, width), ("z", "x", "c"), 0, 0, tiled=True)

    gain = norm_gain[None, :]
    gate, up, down = gate_weight[0], up_weight[0], down_weight[0]
    came, gain2, gate2, up2, down2 = lax.optimization_barrier(
        (came, swap(gain), swap(gate), swap(up), swap(down))
    )
    rows_each = half // CHUNKS
    blocks = call(
        pack_kernel,
        out_shape=[jax.ShapeDtypeStruct((rows_each + PAD, 2 * width), BF)] * CHUNKS,
        in_specs=[SM, VM, VM, VM],
        out_specs=[VM] * CHUNKS,
        compiler_params=pltpu.CompilerParams(vmem_limit_bytes=8 << 20),
        name="pack",
    )(where, came, gain, gain2)

    ff = gate.shape[1]
    wide = [ring(block, count) for block in blocks]
    hidden = [
        call(
            functools.partial(hidden_kernel, count),
            out_shape=jax.ShapeDtypeStruct((rows_each, 2 * ff), BF),
            in_specs=[SM] + [VM] * (count + 4),
            out_specs=VM,
            scratch_shapes=[
                pltpu.VMEM((rows_each, 2 * ff), F32),
                pltpu.VMEM((rows_each, 2 * ff), F32),
                pltpu.VMEM((rows_each, 128), F32),
            ],
            compiler_params=pltpu.CompilerParams(vmem_limit_bytes=24 << 20),
            name="hidden",
        )(where, *found, gate, gate2, up, up2)
        for found in wide
    ]
    wide = [ring(block, count) for block in hidden]

    made = call(
        functools.partial(down_kernel, count),
        out_shape=jax.ShapeDtypeStruct((experts, 2, 8, width), BF),
        in_specs=[SM] + [VM] * (CHUNKS * count + 2),
        out_specs=VM,
        compiler_params=pltpu.CompilerParams(vmem_limit_bytes=24 << 20),
        name="down",
    )(where, *(block for found in wide for block in found), down, down2)
    back = lax.all_to_all(made.reshape(2 * experts, 8, width), ("z", "x", "c"), 0, 0, tiled=True)

    return call(
        functools.partial(combine_kernel, experts, cap),
        out_shape=jax.ShapeDtypeStruct((rows, width), BF),
        in_specs=[VM, VM, VM],
        out_specs=VM,
        compiler_params=pltpu.CompilerParams(vmem_limit_bytes=8 << 20),
        name="combine",
    )(ids, expert_weights.T, back.reshape(experts * cap, width))


def solution(mesh):
    split = Mesh(mesh.devices.reshape(12, 4, 8, 2), ("z", "x", "y", "c"))
    ep, tp = ("z", "x"), ("y", "c")
    in_specs = (
        P(ep, tp),
        P(tp),
        P(ep, None),
        P(ep, None),
        P(ep, None, tp),
        P(ep, None, tp),
        P(ep, None, tp),
    )
    return jax.shard_map(body, mesh=split, in_specs=in_specs, out_specs=P(ep, tp), check_vma=False)
```

```python
import functools

import jax
import jax.numpy as jnp
from jax import lax
from jax.experimental import pallas as pl
from jax.experimental.pallas import tpu as pltpu
from jax.sharding import Mesh, PartitionSpec as P

BF = jnp.bfloat16
F32 = jnp.float32
VM = pl.BlockSpec(memory_space=pltpu.VMEM)
SM = pl.BlockSpec(memory_space=pltpu.SMEM)
PAD = 8


def dot(a, b):
    return jnp.dot(a, b, preferred_element_type=F32)


def dispatch_kernel(experts, cap, ids_ref, tok_ref, out_ref, pick_ref):
    rows = tok_ref.shape[0]
    expert = lax.broadcasted_iota(jnp.int32, (experts, rows), 0)
    named = (expert == ids_ref[0:1, :]) | (expert == ids_ref[1:2, :])
    before = lax.broadcasted_iota(jnp.int32, (rows, rows), 0) < lax.broadcasted_iota(
        jnp.int32, (rows, rows), 1
    )
    rank = dot(named.astype(F32).astype(BF), before.astype(F32).astype(BF))
    rank = jnp.where(named, rank, -1.0)
    slot = lax.broadcasted_iota(jnp.int32, (cap, rows), 0).astype(F32)
    for e in range(experts):
        pick_ref[e * cap : (e + 1) * cap, :] = (
            (rank[e : e + 1, :] == slot).astype(F32).astype(BF)
        )
    out_ref[...] = dot(pick_ref[...], tok_ref[...]).astype(BF)


def combine_kernel(experts, cap, ids_ref, weight_ref, back_ref, out_ref):
    rows = out_ref.shape[0]
    line = lax.broadcasted_iota(jnp.int32, (8, rows), 0)
    table = jnp.where(line == 0, ids_ref[0:1, :].astype(F32), 0.0)
    table = jnp.where(line == 1, ids_ref[1:2, :].astype(F32), table)
    table = jnp.where(line == 2, weight_ref[0:1, :], table)
    table = jnp.where(line == 3, weight_ref[1:2, :], table)
    column = table.T
    first, second = column[:, 0:1], column[:, 1:2]
    lanes = lax.broadcasted_iota(jnp.int32, (rows, 128), 1).astype(F32)
    named = (lanes == first) | (lanes == second)
    after = lax.broadcasted_iota(jnp.int32, (rows, rows), 1) < lax.broadcasted_iota(
        jnp.int32, (rows, rows), 0
    )
    rank = dot(after.astype(F32).astype(BF), named.astype(F32).astype(BF))
    place = lax.broadcasted_iota(jnp.int32, (rows, experts * cap), 1).astype(F32)
    total = None
    for k, name in enumerate((first, second)):
        mine = jnp.sum(jnp.where(lanes == name, rank, 0.0), axis=1, keepdims=True)
        pick = (place == name * cap + mine).astype(F32).astype(BF)
        term = dot(pick, back_ref[...]) * column[:, 2 + k : 3 + k]
        total = term if total is None else total + term
    out_ref[...] = total.astype(BF)


def pack_kernel(where_ref, came_ref, gain_ref, peer_gain_ref, own_ref, pair_ref):
    width = came_ref.shape[2]
    sources = came_ref.shape[0] // 2
    core = where_ref[1]
    mine, other = gain_ref[...], peer_gain_ref[...]
    gain = jnp.concatenate(
        [jnp.where(core == 0, mine, other), jnp.where(core == 0, other, mine)], axis=1
    )
    top = gain.astype(BF).astype(F32)
    mid = (gain - top).astype(BF).astype(F32)
    low = gain - top - mid
    line = lax.broadcasted_iota(jnp.int32, (PAD, 2 * width), 0)
    split = jnp.where(line == 0, top, jnp.where(line == 1, mid, jnp.where(line == 2, low, 0.0)))
    for out_ref in (own_ref, pair_ref.at[0]):
        for s in range(sources):
            for c in range(2):
                out_ref[s * 8 : s * 8 + 8, c * width : (c + 1) * width] = came_ref[2 * s + c]
        out_ref[sources * 8 : sources * 8 + PAD, :] = split.astype(BF)


def origins(where_ref, count):
    here, core = where_ref[0], where_ref[1]

    def partner(y, odd):
        return lax.rem(((y + odd) ^ 1) - odd + count, count)

    def first(y):
        return partner(y, core)

    def second(y):
        return partner(y, 1 - core)

    found = [here, first(here)]
    base = second(here)
    found += [base, first(base)]
    base = second(first(here))
    found += [base, first(base)]
    base = second(first(second(here)))
    found += [base, first(base)]
    return found


def take(refs, sizes):
    parts, at = [], 0
    for size in sizes:
        parts.append(refs[at : at + size])
        at += size
    return parts


def blocks_of(refs):
    return [ref if len(ref.shape) == 2 else ref.at[i] for ref in refs for i in range(1 if len(ref.shape) == 2 else 2)]


def hidden_kernel(count, skip, inputs, last, where_ref, *refs):
    kept = 3 if skip else 0
    blocks, weights, before, outs = take(refs, (inputs, 4, kept, len(refs) - inputs - 4 - kept))
    gate_ref, gate2_ref, up_ref, up2_ref = weights
    blocks = blocks_of(blocks)
    depth = blocks[0].shape[1]
    rows, half = blocks[0].shape[0] - PAD, gate_ref.shape[1]
    total = [ref[...] for ref in before] if skip else None
    places = origins(where_ref, count)[skip : skip + len(blocks)]
    for place, block in zip(places, blocks):
        start = pl.multiple_of(place * depth, depth)
        gain = jnp.sum(block[rows : rows + PAD, :].astype(F32), axis=0, keepdims=True)
        raw = block[0:rows, :].astype(F32)
        squares = raw * raw
        part = squares[:, 0:128]
        for lane in range(128, depth, 128):
            part = part + squares[:, lane : lane + 128]
        scaled = (raw * gain).astype(BF)
        gate = jnp.concatenate([gate_ref[pl.ds(start, depth), :], gate2_ref[pl.ds(start, depth), :]], axis=1)
        up = jnp.concatenate([up_ref[pl.ds(start, depth), :], up2_ref[pl.ds(start, depth), :]], axis=1)
        new = [dot(scaled, gate), dot(scaled, up), part]
        total = new if total is None else [t + n for t, n in zip(total, new)]
    if not last:
        for ref, value in zip(outs, total):
            ref[...] = value
        return
    mean = jnp.sum(total[2], axis=1, keepdims=True) / (depth * count)
    scale = lax.rsqrt(mean + 1e-06)
    gate, up = total[0] * scale, total[1] * scale
    hidden = (gate / (1.0 + jnp.exp(-gate)) * up).astype(BF)
    core = where_ref[1]
    for ref in (outs[0], outs[1].at[0]):
        ref[:, pl.ds(pl.multiple_of(core * half, half), half)] = hidden[:, :half]
        ref[:, pl.ds(pl.multiple_of((1 - core) * half, half), half)] = hidden[:, half:]


def down_kernel(count, skip, inputs, last, where_ref, *refs):
    kept = 2 if skip else 0
    blocks, weights, before, outs = take(refs, (inputs, 2, kept, len(refs) - inputs - 2 - kept))
    blocks = blocks_of(blocks)
    rows, depth = blocks[0].shape
    total = [ref[...] for ref in before] if skip else None
    places = origins(where_ref, count)[skip : skip + len(blocks)]
    for place, block in zip(places, blocks):
        start = pl.multiple_of(place * depth, depth)
        new = [dot(block[...], ref[pl.ds(start, depth), :]) for ref in weights]
        total = new if total is None else [t + n for t, n in zip(total, new)]
    if not last:
        for ref, value in zip(outs, total):
            ref[...] = value
        return
    core = where_ref[1]
    for s in range(rows // 8):
        outs[0][s, core] = total[0][s * 8 : s * 8 + 8, :].astype(BF)
        outs[0][s, 1 - core] = total[1][s * 8 : s * 8 + 8, :].astype(BF)


def gather(own, pair, count):
    def exchange(value, turn):
        perm = []
        for y in range(count):
            for c in range(2):
                odd = (turn + c) % 2
                perm.append((y * 2 + c, (((y + odd) ^ 1) - odd + count) % count * 2 + c))
        return lax.ppermute(value, ("y", "c"), perm)

    got = exchange(own, 0)
    pair = pair.at[1].set(got)
    second = exchange(pair, 1)
    third = exchange(second, 0)
    return [own, got, second], [third], [exchange(third, 1)]


def swap(value):
    return lax.ppermute(value, "c", [(0, 1), (1, 0)])


def body(tokens, norm_gain, expert_ids, expert_weights, gate_weight, up_weight, down_weight):
    count = lax.axis_size("y")
    experts = lax.axis_size("z") * lax.axis_size("x")
    rows, width = tokens.shape
    cap = 3 * rows * expert_ids.shape[1] // (2 * experts)
    half = experts * cap // 2
    where = jnp.stack([lax.axis_index("y"), lax.axis_index("c")]).astype(jnp.int32)
    ids = expert_ids.T
    call = pl.pallas_call

    outgoing = call(
        functools.partial(dispatch_kernel, experts, cap),
        out_shape=jax.ShapeDtypeStruct((experts * cap, width), BF),
        in_specs=[VM, VM],
        out_specs=VM,
        scratch_shapes=[pltpu.VMEM((experts * cap, rows), BF)],
        name="dispatch",
    )(ids, tokens)
    came = lax.all_to_all(outgoing.reshape(2 * experts, 8, width), ("z", "x", "c"), 0, 0, tiled=True)

    gain = norm_gain[None, :]
    gate, up, down = gate_weight[0], up_weight[0], down_weight[0]
    came, gain2, gate2, up2, down2 = lax.optimization_barrier(
        (came, swap(gain), swap(gate), swap(up), swap(down))
    )
    packed = (half + PAD, 2 * width)
    own, pair = call(
        pack_kernel,
        out_shape=[jax.ShapeDtypeStruct(packed, BF), jax.ShapeDtypeStruct((2, *packed), BF)],
        in_specs=[SM, VM, VM, VM],
        out_specs=[VM, VM],
        compiler_params=pltpu.CompilerParams(vmem_limit_bytes=8 << 20),
        name="pack",
    )(where, came, gain, gain2)

    def product(kernel, name, groups, weights, sums, outs, each):
        total, skip = [], 0
        for number, group in enumerate(groups):
            last = number == len(groups) - 1
            blocks = sum(1 if block.ndim == 2 else 2 for block in group)
            shapes = outs if last else sums
            total = call(
                functools.partial(kernel, count, skip, len(group), last),
                out_shape=shapes,
                in_specs=[SM] + [VM] * (len(group) + len(weights) + len(total)),
                out_specs=[VM] * len(shapes),
                compiler_params=pltpu.CompilerParams(vmem_limit_bytes=16 << 20),
                cost_estimate=pl.CostEstimate(
                    flops=blocks * each, bytes_accessed=blocks * each // 512, transcendentals=0
                ),
                name=name,
            )(where, *group, *weights, *total)
            skip += blocks
        return total

    ff = gate.shape[1]
    own, pair = product(
        hidden_kernel,
        "hidden",
        gather(own, pair, count),
        (gate, gate2, up, up2),
        [jax.ShapeDtypeStruct((half, 2 * ff), F32)] * 2 + [jax.ShapeDtypeStruct((half, 128), F32)],
        [jax.ShapeDtypeStruct((half, 2 * ff), BF), jax.ShapeDtypeStruct((2, half, 2 * ff), BF)],
        2 * half * 2 * width * 4 * ff,
    )
    (made,) = product(
        down_kernel,
        "down",
        gather(own, pair, count),
        (down, down2),
        [jax.ShapeDtypeStruct((half, width), F32)] * 2,
        [jax.ShapeDtypeStruct((experts, 2, 8, width), BF)],
        2 * half * 2 * ff * 2 * width,
    )
    back = lax.all_to_all(made.reshape(2 * experts, 8, width), ("z", "x", "c"), 0, 0, tiled=True)

    return call(
        functools.partial(combine_kernel, experts, cap),
        out_shape=jax.ShapeDtypeStruct((rows, width), BF),
        in_specs=[VM, VM, VM],
        out_specs=VM,
        compiler_params=pltpu.CompilerParams(vmem_limit_bytes=8 << 20),
        name="combine",
    )(ids, expert_weights.T, back.reshape(experts * cap, width))


def solution(mesh):
    split = Mesh(mesh.devices.reshape(12, 4, 8, 2), ("z", "x", "y", "c"))
    ep, tp = ("z", "x"), ("y", "c")
    in_specs = (
        P(ep, tp),
        P(tp),
        P(ep, None),
        P(ep, None),
        P(ep, None, tp),
        P(ep, None, tp),
        P(ep, None, tp),
    )
    return jax.shard_map(body, mesh=split, in_specs=in_specs, out_specs=P(ep, tp), check_vma=False)
```

```python
import functools

import jax
import jax.numpy as jnp
from jax import lax
from jax.experimental import pallas as pl
from jax.experimental.pallas import tpu as pltpu
from jax.sharding import Mesh, PartitionSpec as P

BF = jnp.bfloat16
F32 = jnp.float32
VM = pl.BlockSpec(memory_space=pltpu.VMEM)
SM = pl.BlockSpec(memory_space=pltpu.SMEM)
PAD = 8
LANES = 128
QUART = 4


def dot(a, b):
    return jnp.dot(a, b, preferred_element_type=F32)


def ones_where(mask):
    return mask.astype(F32).astype(BF)


def dispatch_kernel(experts, cap, ids_ref, tok_ref, out_ref, pick_ref):
    rows = tok_ref.shape[0]
    expert = lax.broadcasted_iota(jnp.int32, (experts, rows), 0)
    named = (expert == ids_ref[0:1, :]) | (expert == ids_ref[1:2, :])
    before = lax.broadcasted_iota(jnp.int32, (rows, rows), 0) < lax.broadcasted_iota(
        jnp.int32, (rows, rows), 1
    )
    rank = jnp.where(named, dot(ones_where(named), ones_where(before)), -1.0)
    line = lax.broadcasted_iota(jnp.int32, (2 * cap, 2 * rows), 0)
    column = lax.broadcasted_iota(jnp.int32, (2 * cap, 2 * rows), 1)
    slot = line // 8 * QUART + line % QUART
    wanted = jnp.where(line % 8 // QUART == column // rows, slot, -2).astype(F32)
    rank2 = jnp.concatenate([rank, rank], axis=1)
    for e in range(experts):
        pick_ref[e * 2 * cap : (e + 1) * 2 * cap, :] = ones_where(rank2[e : e + 1, :] == wanted)
    halves = jnp.concatenate([tok_ref[:, :LANES], tok_ref[:, LANES:]], axis=0)
    out_ref[...] = dot(pick_ref[...], halves).astype(BF)


def combine_kernel(experts, cap, ids_ref, weight_ref, back_ref, out_ref):
    rows = out_ref.shape[0]
    line = lax.broadcasted_iota(jnp.int32, (8, rows), 0)
    table = jnp.where(line == 0, ids_ref[0:1, :].astype(F32), 0.0)
    table = jnp.where(line == 1, ids_ref[1:2, :].astype(F32), table)
    table = jnp.where(line == 2, weight_ref[0:1, :], table)
    table = jnp.where(line == 3, weight_ref[1:2, :], table)
    column = table.T
    first, second = column[:, 0:1], column[:, 1:2]
    lanes = lax.broadcasted_iota(jnp.int32, (rows, LANES), 1).astype(F32)
    named = (lanes == first) | (lanes == second)
    after = lax.broadcasted_iota(jnp.int32, (rows, rows), 1) < lax.broadcasted_iota(
        jnp.int32, (rows, rows), 0
    )
    rank = dot(ones_where(after), ones_where(named))
    place = lax.broadcasted_iota(jnp.int32, (rows, experts * 2 * cap), 1).astype(F32)
    total = [None, None]
    for k, name in enumerate((first, second)):
        mine = jnp.sum(jnp.where(lanes == name, rank, 0.0), axis=1, keepdims=True)
        at = name * (2 * cap) + jnp.floor(mine / QUART) * QUART + mine
        for half in range(2):
            pick = ones_where(place == at + half * QUART)
            term = dot(pick, back_ref[...]) * column[:, 2 + k : 3 + k]
            total[half] = term if k == 0 else total[half] + term
    out_ref[:, :LANES] = total[0].astype(BF)
    out_ref[:, LANES:] = total[1].astype(BF)


def trade(a, b):
    top = lax.broadcasted_iota(jnp.int32, a.shape, 0) < QUART
    return jnp.where(top, a, pltpu.roll(b, QUART, 0)), jnp.where(top, pltpu.roll(a, QUART, 0), b)


def pack_kernel(came_ref, gain_ref, *out_refs):
    sources = came_ref.shape[0] // len(out_refs)
    parts = came_ref.shape[1]
    for number, out_ref in enumerate(out_refs):
        for s in range(0, sources, 2):
            for part in range(parts):
                a = came_ref[number * sources + s, part].astype(F32)
                b = came_ref[number * sources + s + 1, part].astype(F32)
                for half, tile in enumerate(trade(a, b)):
                    at = (2 * part + half) * LANES
                    out_ref[s * QUART : s * QUART + 8, at : at + LANES] = tile.astype(BF)
    gain = jnp.concatenate([gain_ref[i : i + 1, :] for i in range(parts)], axis=1)
    top = gain.astype(BF).astype(F32)
    mid = (gain - top).astype(BF).astype(F32)
    low = gain - top - mid
    line = lax.broadcasted_iota(jnp.int32, (PAD, gain.shape[1]), 0)
    split = jnp.where(line == 0, top, jnp.where(line == 1, mid, jnp.where(line == 2, low, 0.0)))
    out_refs[0][sources * QUART :, :] = split.astype(BF)


def positions(where_ref):
    chip, core = where_ref[0], where_ref[1]
    return [chip * 2 + core, chip * 2 + 1 - core, (1 - chip) * 2 + core, (1 - chip) * 2 + 1 - core]


def hidden_kernel(where_ref, a_ref, b_ref, *refs):
    gates, ups, out_ref = refs[:4], refs[4:8], refs[8]
    blocks, _, depth = a_ref.shape
    half, piece = b_ref.shape[1], gates[0].shape[1]
    square, sums = None, [None] * 4
    for q in range(blocks):
        gain = jnp.sum(a_ref[q, half:, :].astype(F32), axis=0, keepdims=True)
        raw = jnp.concatenate([a_ref[q, :half, :].astype(F32), b_ref[q].astype(F32)], axis=0)
        squares = raw * raw
        part = squares[:, :LANES]
        for lane in range(LANES, depth, LANES):
            part = part + squares[:, lane : lane + LANES]
        square = part if q == 0 else square + part
        scaled = (raw * gain).astype(BF)
        for i, (first, second) in enumerate((gates[:2], ups[:2], gates[2:], ups[2:])):
            span = slice(q * depth, (q + 1) * depth)
            new = dot(scaled, jnp.concatenate([first[span, :], second[span, :]], axis=1))
            sums[i] = new if q == 0 else sums[i] + new
    mean = jnp.sum(square, axis=1, keepdims=True) / (depth * blocks)
    scale = lax.rsqrt(mean + 1e-06)
    place = positions(where_ref)
    for i in range(2):
        gate, up = sums[2 * i] * scale, sums[2 * i + 1] * scale
        hidden = (gate / (1.0 + jnp.exp(-gate)) * up).astype(BF)
        for j in range(2):
            at = pl.multiple_of(place[2 * i + j] * piece, piece)
            out_ref[:, pl.ds(at, piece)] = hidden[:, j * piece : (j + 1) * piece]


def down_kernel(where_ref, hidden_ref, *refs):
    downs, out_ref = refs[:4], refs[4]
    blocks, rows, depth = hidden_ref.shape
    for place, down in zip(positions(where_ref), downs):
        total = None
        for q in range(blocks):
            new = dot(hidden_ref[q], down[q * depth : (q + 1) * depth, :])
            total = new if q == 0 else total + new
        for s in range(0, rows // QUART, 2):
            at = s * QUART
            first, second = trade(total[at : at + 8, :LANES], total[at : at + 8, LANES:])
            out_ref[s, place] = first.astype(BF)
            out_ref[s + 1, place] = second.astype(BF)


def body(tokens, norm_gain, expert_ids, expert_weights, gate_weight, up_weight, down_weight):
    experts = lax.axis_size("z") * lax.axis_size("x")
    parts = lax.axis_size("p") * lax.axis_size("c")
    rows, width = tokens.shape
    cap = 3 * rows * expert_ids.shape[1] // (2 * experts)
    quarter = experts * cap // parts
    where = jnp.stack([lax.axis_index("p"), lax.axis_index("c")]).astype(jnp.int32)
    ids = expert_ids.T
    wide = ("z", "x", "p", "c")

    def params(mib, flops=0):
        return dict(
            compiler_params=pltpu.CompilerParams(vmem_limit_bytes=mib << 20),
            cost_estimate=pl.CostEstimate(flops=flops, bytes_accessed=1 << 20, transcendentals=0),
        )

    def swap(value, axis):
        return lax.ppermute(value, axis, [(0, 1), (1, 0)])

    outgoing = pl.pallas_call(
        functools.partial(dispatch_kernel, experts, cap),
        out_shape=jax.ShapeDtypeStruct((experts * 2 * cap, LANES), BF),
        in_specs=[VM, VM],
        out_specs=VM,
        scratch_shapes=[pltpu.VMEM((experts * 2 * cap, 2 * rows), BF)],
        name="dispatch",
    )(ids, tokens)
    came = lax.all_to_all(outgoing.reshape(experts * parts, 8, LANES), wide, 0, 0, tiled=True)

    own = [gate_weight[0], up_weight[0], down_weight[0]]
    over = [swap(w, "p") for w in own]
    side = [swap(w, "c") for w in own]
    gains = lax.all_gather(norm_gain, ("p", "c"), axis=0)
    came, gains, side = lax.optimization_barrier((came, gains, side))

    one, two = pl.pallas_call(
        pack_kernel,
        out_shape=[
            jax.ShapeDtypeStruct((quarter // 2 + PAD, parts * width), BF),
            jax.ShapeDtypeStruct((quarter // 2, parts * width), BF),
        ],
        in_specs=[VM, VM],
        out_specs=[VM, VM],
        name="pack",
        **params(8),
    )(came.reshape(experts, parts, 8, LANES), gains)
    one = lax.all_gather(one, "q", axis=0)
    one, over[0], over[1] = lax.optimization_barrier((one, over[0], over[1]))
    far = [swap(w, "c") for w in over[:2]]
    two = lax.all_gather(two, "q", axis=0)

    piece = gate_weight.shape[2]
    hidden = pl.pallas_call(
        hidden_kernel,
        out_shape=jax.ShapeDtypeStruct((quarter, parts * piece), BF),
        in_specs=[SM] + [VM] * 10,
        out_specs=VM,
        name="hidden",
        **params(24, 1 << 31),
    )(where, one, two, own[0], side[0], over[0], far[0], own[1], side[1], over[1], far[1])
    hidden, over[2] = lax.optimization_barrier((hidden, over[2]))
    far.append(swap(over[2], "c"))
    hidden = lax.all_gather(hidden, "q", axis=0)

    made = pl.pallas_call(
        down_kernel,
        out_shape=jax.ShapeDtypeStruct((experts, parts, 8, LANES), BF),
        in_specs=[SM] + [VM] * 5,
        out_specs=VM,
        name="down",
        **params(16, 1 << 30),
    )(where, hidden, own[2], side[2], over[2], far[2])
    back = lax.all_to_all(made.reshape(experts * parts, 8, LANES), wide, 0, 0, tiled=True)

    return pl.pallas_call(
        functools.partial(combine_kernel, experts, cap),
        out_shape=jax.ShapeDtypeStruct((rows, width), BF),
        in_specs=[VM, VM, VM],
        out_specs=VM,
        name="combine",
        **params(16),
    )(ids, expert_weights.T, back.reshape(experts * 2 * cap, LANES))


def solution(mesh):
    split = Mesh(mesh.devices.reshape(12, 4, 4, 2, 2), ("z", "x", "q", "p", "c"))
    ep, tp = ("z", "x"), ("q", "p", "c")
    in_specs = (
        P(ep, tp),
        P(tp),
        P(ep, None),
        P(ep, None),
        P(ep, None, tp),
        P(ep, None, tp),
        P(ep, None, tp),
    )
    return jax.shard_map(body, mesh=split, in_specs=in_specs, out_specs=P(ep, tp), check_vma=False)
```

```python
import functools

import jax
import jax.numpy as jnp
from jax import lax
from jax.experimental import pallas as pl
from jax.experimental.pallas import tpu as pltpu
from jax.sharding import Mesh, PartitionSpec as P

BF = jnp.bfloat16
F32 = jnp.float32
VM = pl.BlockSpec(memory_space=pltpu.VMEM)
SM = pl.BlockSpec(memory_space=pltpu.SMEM)
STEPS = (0, 1, -1, 2, -2, 3, -3, 4)
PAD = 8


def dot(a, b):
    return jnp.dot(a, b, preferred_element_type=F32)


def dispatch_kernel(experts, cap, ids_ref, tok_ref, out_ref, pick_ref):
    rows = tok_ref.shape[0]
    expert = lax.broadcasted_iota(jnp.int32, (experts, rows), 0)
    named = (expert == ids_ref[0:1, :]) | (expert == ids_ref[1:2, :])
    before = lax.broadcasted_iota(jnp.int32, (rows, rows), 0) < lax.broadcasted_iota(
        jnp.int32, (rows, rows), 1
    )
    rank = dot(named.astype(F32).astype(BF), before.astype(F32).astype(BF))
    rank = jnp.where(named, rank, -1.0)
    slot = lax.broadcasted_iota(jnp.int32, (cap, rows), 0).astype(F32)
    for e in range(experts):
        pick_ref[e * cap : (e + 1) * cap, :] = (
            (rank[e : e + 1, :] == slot).astype(F32).astype(BF)
        )
    out_ref[...] = dot(pick_ref[...], tok_ref[...]).astype(BF)


def combine_kernel(experts, cap, ids_ref, weight_ref, back_ref, out_ref):
    rows = out_ref.shape[0]
    line = lax.broadcasted_iota(jnp.int32, (8, rows), 0)
    table = jnp.where(line == 0, ids_ref[0:1, :].astype(F32), 0.0)
    table = jnp.where(line == 1, ids_ref[1:2, :].astype(F32), table)
    table = jnp.where(line == 2, weight_ref[0:1, :], table)
    table = jnp.where(line == 3, weight_ref[1:2, :], table)
    column = table.T
    first, second = column[:, 0:1], column[:, 1:2]
    lanes = lax.broadcasted_iota(jnp.int32, (rows, 128), 1).astype(F32)
    named = (lanes == first) | (lanes == second)
    after = lax.broadcasted_iota(jnp.int32, (rows, rows), 1) < lax.broadcasted_iota(
        jnp.int32, (rows, rows), 0
    )
    rank = dot(after.astype(F32).astype(BF), named.astype(F32).astype(BF))
    place = lax.broadcasted_iota(jnp.int32, (rows, experts * cap), 1).astype(F32)
    total = None
    for k, name in enumerate((first, second)):
        mine = jnp.sum(jnp.where(lanes == name, rank, 0.0), axis=1, keepdims=True)
        pick = (place == name * cap + mine).astype(F32).astype(BF)
        term = dot(pick, back_ref[...]) * column[:, 2 + k : 3 + k]
        total = term if total is None else total + term
    out_ref[...] = total.astype(BF)


def pack_kernel(where_ref, came_ref, gain_ref, peer_gain_ref, out_ref):
    sources = came_ref.shape[0] // 2
    width = came_ref.shape[2]
    for s in range(sources):
        for c in range(2):
            out_ref[s * 8 : s * 8 + 8, c * width : (c + 1) * width] = came_ref[2 * s + c]
    core = where_ref[1]
    mine, other = gain_ref[...], peer_gain_ref[...]
    gain = jnp.concatenate(
        [jnp.where(core == 0, mine, other), jnp.where(core == 0, other, mine)], axis=1
    )
    top = gain.astype(BF).astype(F32)
    mid = (gain - top).astype(BF).astype(F32)
    low = gain - top - mid
    line = lax.broadcasted_iota(jnp.int32, (PAD, 2 * width), 0)
    split = jnp.where(line == 0, top, jnp.where(line == 1, mid, jnp.where(line == 2, low, 0.0)))
    out_ref[sources * 8 : sources * 8 + PAD, :] = split.astype(BF)


def source_of(where_ref, step, count):
    turn = 1 - 2 * where_ref[1]
    return lax.rem(where_ref[0] - step * turn + 2 * count, count)


def hidden_kernel(count, where_ref, *refs):
    blocks, (gate_ref, gate2_ref, up_ref, up2_ref, out_ref, gsum, usum, square) = refs[:8], refs[8:]
    rows, half = out_ref.shape[0], gate_ref.shape[1]
    depth = blocks[0].shape[1]
    for number, (step, block) in enumerate(zip(STEPS, blocks)):
        start = pl.multiple_of(source_of(where_ref, step, count) * depth, depth)
        gain = jnp.sum(block[rows : rows + PAD, :].astype(F32), axis=0, keepdims=True)
        raw = block[0:rows, :].astype(F32)
        squares = raw * raw
        part = squares[:, 0:128]
        for lane in range(128, depth, 128):
            part = part + squares[:, lane : lane + 128]
        scaled = (raw * gain).astype(BF)
        gate = jnp.concatenate([gate_ref[pl.ds(start, depth), :], gate2_ref[pl.ds(start, depth), :]], axis=1)
        up = jnp.concatenate([up_ref[pl.ds(start, depth), :], up2_ref[pl.ds(start, depth), :]], axis=1)
        if number == 0:
            square[...] = part
            gsum[...] = dot(scaled, gate)
            usum[...] = dot(scaled, up)
        else:
            square[...] += part
            gsum[...] += dot(scaled, gate)
            usum[...] += dot(scaled, up)
    mean = jnp.sum(square[...], axis=1, keepdims=True) / (depth * count)
    scale = lax.rsqrt(mean + 1e-06)
    gate, up = gsum[...] * scale, usum[...] * scale
    hidden = (gate / (1.0 + jnp.exp(-gate)) * up).astype(BF)
    core = where_ref[1]
    out_ref[:, pl.ds(pl.multiple_of(core * half, half), half)] = hidden[:, :half]
    out_ref[:, pl.ds(pl.multiple_of((1 - core) * half, half), half)] = hidden[:, half:]


def down_kernel(count, where_ref, *refs):
    blocks, (down_ref, down2_ref, out_ref, mine, other) = refs[:8], refs[8:]
    depth = blocks[0].shape[1]
    for number, (step, block) in enumerate(zip(STEPS, blocks)):
        start = pl.multiple_of(source_of(where_ref, step, count) * depth, depth)
        first = dot(block[...], down_ref[pl.ds(start, depth), :])
        second = dot(block[...], down2_ref[pl.ds(start, depth), :])
        if number == 0:
            mine[...] = first
            other[...] = second
        else:
            mine[...] += first
            other[...] += second
    core = where_ref[1]
    for s in range(out_ref.shape[0]):
        out_ref[s, core] = mine[s * 8 : s * 8 + 8, :].astype(BF)
        out_ref[s, 1 - core] = other[s * 8 : s * 8 + 8, :].astype(BF)


def ring(block, count):
    def perm(sign):
        return [
            (y * 2 + c, (y + sign * (1 - 2 * c)) % count * 2 + c) for y in range(count) for c in range(2)
        ]

    main = other = block
    found = [block]
    for k in range(3):
        main = lax.ppermute(main, ("y", "c"), perm(1))
        other = lax.ppermute(other, ("y", "c"), perm(-1))
        found += [main, other]
    found.append(lax.ppermute(main, ("y", "c"), perm(1)))
    return found


def swap(value):
    return lax.ppermute(value, "c", [(0, 1), (1, 0)])


def body(tokens, norm_gain, expert_ids, expert_weights, gate_weight, up_weight, down_weight):
    count = lax.axis_size("y")
    experts = lax.axis_size("z") * lax.axis_size("x")
    rows, width = tokens.shape
    cap = 3 * rows * expert_ids.shape[1] // (2 * experts)
    half = experts * cap // 2
    where = jnp.stack([lax.axis_index("y"), lax.axis_index("c")]).astype(jnp.int32)
    ids = expert_ids.T
    call = pl.pallas_call

    outgoing = call(
        functools.partial(dispatch_kernel, experts, cap),
        out_shape=jax.ShapeDtypeStruct((experts * cap, width), BF),
        in_specs=[VM, VM],
        out_specs=VM,
        scratch_shapes=[pltpu.VMEM((experts * cap, rows), BF)],
        name="dispatch",
    )(ids, tokens)
    came = lax.all_to_all(outgoing.reshape(2 * experts, 8, width), ("z", "x", "c"), 0, 0, tiled=True)

    gain = norm_gain[None, :]
    gate, up, down = gate_weight[0], up_weight[0], down_weight[0]
    came, gain2, gate2, up2, down2 = lax.optimization_barrier(
        (came, swap(gain), swap(gate), swap(up), swap(down))
    )
    block = call(
        pack_kernel,
        out_shape=jax.ShapeDtypeStruct((half + PAD, 2 * width), BF),
        in_specs=[SM, VM, VM, VM],
        out_specs=VM,
        compiler_params=pltpu.CompilerParams(vmem_limit_bytes=8 << 20),
        name="pack",
    )(where, came, gain, gain2)
    found = ring(block, count)

    ff = gate.shape[1]
    hidden = call(
        functools.partial(hidden_kernel, count),
        out_shape=jax.ShapeDtypeStruct((half, 2 * ff), BF),
        in_specs=[SM] + [VM] * 12,
        out_specs=VM,
        scratch_shapes=[
            pltpu.VMEM((half, 2 * ff), F32),
            pltpu.VMEM((half, 2 * ff), F32),
            pltpu.VMEM((half, 128), F32),
        ],
        compiler_params=pltpu.CompilerParams(vmem_limit_bytes=12 << 20),
        name="hidden",
    )(where, *found, gate, gate2, up, up2)
    found = ring(hidden, count)

    made = call(
        functools.partial(down_kernel, count),
        out_shape=jax.ShapeDtypeStruct((experts, 2, 8, width), BF),
        in_specs=[SM] + [VM] * 10,
        out_specs=VM,
        scratch_shapes=[pltpu.VMEM((half, width), F32), pltpu.VMEM((half, width), F32)],
        compiler_params=pltpu.CompilerParams(vmem_limit_bytes=12 << 20),
        name="down",
    )(where, *found, down, down2)
    back = lax.all_to_all(made.reshape(2 * experts, 8, width), ("z", "x", "c"), 0, 0, tiled=True)

    return call(
        functools.partial(combine_kernel, experts, cap),
        out_shape=jax.ShapeDtypeStruct((rows, width), BF),
        in_specs=[VM, VM, VM],
        out_specs=VM,
        compiler_params=pltpu.CompilerParams(vmem_limit_bytes=8 << 20),
        name="combine",
    )(ids, expert_weights.T, back.reshape(experts * cap, width))


def solution(mesh):
    split = Mesh(mesh.devices.reshape(12, 4, 8, 2), ("z", "x", "y", "c"))
    ep, tp = ("z", "x"), ("y", "c")
    in_specs = (
        P(ep, tp),
        P(tp),
        P(ep, None),
        P(ep, None),
        P(ep, None, tp),
        P(ep, None, tp),
        P(ep, None, tp),
    )
    return jax.shard_map(body, mesh=split, in_specs=in_specs, out_specs=P(ep, tp), check_vma=False)
```

```python
import functools

import jax
import jax.numpy as jnp
from jax import lax
from jax.experimental import pallas as pl
from jax.experimental.pallas import tpu as pltpu
from jax.sharding import Mesh, PartitionSpec as P

BF = jnp.bfloat16
F32 = jnp.float32
VM = pl.BlockSpec(memory_space=pltpu.VMEM)
STEPS = (0, 1, -1, 2, -2, 3, -3, 4)
PAD = 8


def dot(a, b):
    return jnp.dot(a, b, preferred_element_type=F32)


def dispatch_kernel(experts, cap, ids_ref, tok_ref, out_ref, pick_ref):
    rows = tok_ref.shape[0]
    expert = lax.broadcasted_iota(jnp.int32, (experts, rows), 0)
    named = (expert == ids_ref[0:1, :]) | (expert == ids_ref[1:2, :])
    before = lax.broadcasted_iota(jnp.int32, (rows, rows), 0) < lax.broadcasted_iota(
        jnp.int32, (rows, rows), 1
    )
    rank = dot(named.astype(F32).astype(BF), before.astype(F32).astype(BF))
    rank = jnp.where(named, rank, -1.0)
    slot = lax.broadcasted_iota(jnp.int32, (cap, rows), 0).astype(F32)
    for e in range(experts):
        pick_ref[e * cap : (e + 1) * cap, :] = (
            (rank[e : e + 1, :] == slot).astype(F32).astype(BF)
        )
    out_ref[...] = dot(pick_ref[...], tok_ref[...]).astype(BF)


def plan_kernel(experts, cap, ids_ref, weight_ref, pick_ref, share_ref):
    rows = pick_ref.shape[1]
    line = lax.broadcasted_iota(jnp.int32, (8, rows), 0)
    table = jnp.where(line == 0, ids_ref[0:1, :].astype(F32), 0.0)
    table = jnp.where(line == 1, ids_ref[1:2, :].astype(F32), table)
    table = jnp.where(line == 2, weight_ref[0:1, :], table)
    table = jnp.where(line == 3, weight_ref[1:2, :], table)
    column = table.T
    first, second = column[:, 0:1], column[:, 1:2]
    lanes = lax.broadcasted_iota(jnp.int32, (rows, 128), 1).astype(F32)
    named = (lanes == first) | (lanes == second)
    after = lax.broadcasted_iota(jnp.int32, (rows, rows), 1) < lax.broadcasted_iota(
        jnp.int32, (rows, rows), 0
    )
    rank = dot(after.astype(F32).astype(BF), named.astype(F32).astype(BF))
    place = lax.broadcasted_iota(jnp.int32, (rows, experts * cap), 1).astype(F32)
    for k, name in enumerate((first, second)):
        mine = jnp.sum(jnp.where(lanes == name, rank, 0.0), axis=1, keepdims=True)
        pick_ref[k] = (place == name * cap + mine).astype(F32).astype(BF)
        share_ref[k] = jnp.broadcast_to(column[:, 2 + k : 3 + k], (rows, 128))


def combine_kernel(pick_ref, share_ref, back_ref, out_ref):
    total = None
    for k in range(2):
        term = dot(pick_ref[k], back_ref[...]) * share_ref[k][:, :1]
        total = term if k == 0 else total + term
    out_ref[...] = total.astype(BF)


def pack_kernel(came_ref, gain_ref, out_ref):
    sources = came_ref.shape[0] // 2
    width = came_ref.shape[2]
    for s in range(sources):
        for c in range(2):
            out_ref[s * 8 : s * 8 + 8, c * width : (c + 1) * width] = came_ref[2 * s + c]
    gain = jnp.concatenate([gain_ref[0], gain_ref[1]], axis=1)
    top = gain.astype(BF).astype(F32)
    mid = (gain - top).astype(BF).astype(F32)
    low = gain - top - mid
    line = lax.broadcasted_iota(jnp.int32, (PAD, 2 * width), 0)
    split = jnp.where(line == 0, top, jnp.where(line == 1, mid, jnp.where(line == 2, low, 0.0)))
    out_ref[sources * 8 : sources * 8 + PAD, :] = split.astype(BF)


def source_of(step, count):
    turn = 1 - 2 * lax.axis_index("c")
    return lax.rem(lax.axis_index("y") - step * turn + 2 * count, count)


def take(refs, sizes):
    parts, at = [], 0
    for size in sizes:
        parts.append(refs[at : at + size])
        at += size
    return parts


def hidden_kernel(count, skip, inputs, last, *refs):
    kept = 3 if skip else 0
    blocks, weights, before, outs = take(refs, (inputs, 4, kept, len(refs) - inputs - 4 - kept))
    gate_ref, gate2_ref, up_ref, up2_ref = weights
    depth = blocks[0].shape[1]
    rows, half = blocks[0].shape[0] - PAD, gate_ref.shape[1]
    total = [ref[...] for ref in before] if skip else None
    for step, block in zip(STEPS[skip : skip + inputs], blocks):
        start = pl.multiple_of(source_of(step, count) * depth, depth)
        gain = jnp.sum(block[rows : rows + PAD, :].astype(F32), axis=0, keepdims=True)
        raw = block[0:rows, :].astype(F32)
        squares = raw * raw
        part = squares[:, 0:128]
        for lane in range(128, depth, 128):
            part = part + squares[:, lane : lane + 128]
        scaled = (raw * gain).astype(BF)
        gate = jnp.concatenate([gate_ref[pl.ds(start, depth), :], gate2_ref[pl.ds(start, depth), :]], axis=1)
        up = jnp.concatenate([up_ref[pl.ds(start, depth), :], up2_ref[pl.ds(start, depth), :]], axis=1)
        new = [dot(scaled, gate), dot(scaled, up), part]
        total = new if total is None else [t + n for t, n in zip(total, new)]
    if not last:
        for ref, value in zip(outs, total):
            ref[...] = value
        return
    mean = jnp.sum(total[2], axis=1, keepdims=True) / (depth * count)
    scale = lax.rsqrt(mean + 1e-06)
    gate, up = total[0] * scale, total[1] * scale
    hidden = (gate / (1.0 + jnp.exp(-gate)) * up).astype(BF)
    core = lax.axis_index("c")
    outs[0][:, pl.ds(pl.multiple_of(core * half, half), half)] = hidden[:, :half]
    outs[0][:, pl.ds(pl.multiple_of((1 - core) * half, half), half)] = hidden[:, half:]


def down_kernel(count, skip, inputs, last, *refs):
    kept = 2 if skip else 0
    blocks, weights, before, outs = take(refs, (inputs, 2, kept, len(refs) - inputs - 2 - kept))
    rows, depth = blocks[0].shape
    total = [ref[...] for ref in before] if skip else None
    for step, block in zip(STEPS[skip : skip + inputs], blocks):
        start = pl.multiple_of(source_of(step, count) * depth, depth)
        new = [dot(block[...], ref[pl.ds(start, depth), :]) for ref in weights]
        total = new if total is None else [t + n for t, n in zip(total, new)]
    if not last:
        for ref, value in zip(outs, total):
            ref[...] = value
        return
    core = lax.axis_index("c")
    for s in range(rows // 8):
        outs[0][s, core] = total[0][s * 8 : s * 8 + 8, :].astype(BF)
        outs[0][s, 1 - core] = total[1][s * 8 : s * 8 + 8, :].astype(BF)


def ring(block, count):
    def perm(sign):
        return [
            (y * 2 + c, (y + sign * (1 - 2 * c)) % count * 2 + c) for y in range(count) for c in range(2)
        ]

    main = other = block
    found = [block]
    for k in range(3):
        main = lax.ppermute(main, ("y", "c"), perm(1))
        other = lax.ppermute(other, ("y", "c"), perm(-1))
        found += [main, other]
    found.append(lax.ppermute(main, ("y", "c"), perm(1)))
    return found


def swap(value):
    return lax.ppermute(value, "c", [(0, 1), (1, 0)])


def body(tokens, norm_gain, expert_ids, expert_weights, gate_weight, up_weight, down_weight):
    count = lax.axis_size("y")
    experts = lax.axis_size("z") * lax.axis_size("x")
    rows, width = tokens.shape
    cap = 3 * rows * expert_ids.shape[1] // (2 * experts)
    half = experts * cap // 2
    ids = expert_ids.T
    call = pl.pallas_call

    outgoing = call(
        functools.partial(dispatch_kernel, experts, cap),
        out_shape=jax.ShapeDtypeStruct((experts * cap, width), BF),
        in_specs=[VM, VM],
        out_specs=VM,
        scratch_shapes=[pltpu.VMEM((experts * cap, rows), BF)],
        name="dispatch",
    )(ids, tokens)
    came = lax.all_to_all(outgoing.reshape(2 * experts, 8, width), ("z", "x", "c"), 0, 0, tiled=True)

    picks, shares = call(
        functools.partial(plan_kernel, experts, cap),
        out_shape=[
            jax.ShapeDtypeStruct((2, rows, experts * cap), BF),
            jax.ShapeDtypeStruct((2, rows, 128), F32),
        ],
        in_specs=[VM, VM],
        out_specs=[VM, VM],
        compiler_params=pltpu.CompilerParams(vmem_limit_bytes=8 << 20),
        cost_estimate=pl.CostEstimate(flops=1 << 30, bytes_accessed=1 << 20, transcendentals=0),
        name="plan",
    )(ids, expert_weights.T)
    gate, up, down = gate_weight[0], up_weight[0], down_weight[0]
    came, gains, gate2, up2, down2, picks, shares = lax.optimization_barrier(
        (came, lax.all_gather(norm_gain[None], "c", axis=0), swap(gate), swap(up), swap(down), picks, shares)
    )
    block = call(
        pack_kernel,
        out_shape=jax.ShapeDtypeStruct((half + PAD, 2 * width), BF),
        in_specs=[VM, VM],
        out_specs=VM,
        compiler_params=pltpu.CompilerParams(vmem_limit_bytes=8 << 20),
        name="pack",
    )(came, gains)

    def product(kernel, name, found, weights, sums, outs, each):
        total, skip = [], 0
        for group in (found,):
            last = skip + len(group) == count
            shapes = outs if last else sums
            total = call(
                functools.partial(kernel, count, skip, len(group), last),
                out_shape=shapes,
                in_specs=[VM] * (len(group) + len(weights) + len(total)),
                out_specs=[VM] * len(shapes),
                compiler_params=pltpu.CompilerParams(vmem_limit_bytes=16 << 20),
                cost_estimate=pl.CostEstimate(
                    flops=len(group) * each, bytes_accessed=1 << 20, transcendentals=0
                ),
                name=name,
            )(*group, *weights, *total)
            skip += len(group)
        return total

    ff = gate.shape[1]
    (hidden,) = product(
        hidden_kernel,
        "hidden",
        ring(block, count),
        (gate, gate2, up, up2),
        [jax.ShapeDtypeStruct((half, 2 * ff), F32)] * 2 + [jax.ShapeDtypeStruct((half, 128), F32)],
        [jax.ShapeDtypeStruct((half, 2 * ff), BF)],
        2 * half * 2 * width * 4 * ff,
    )
    (made,) = product(
        down_kernel,
        "down",
        ring(hidden, count),
        (down, down2),
        [jax.ShapeDtypeStruct((half, width), F32)] * 2,
        [jax.ShapeDtypeStruct((experts, 2, 8, width), BF)],
        2 * half * 2 * ff * 2 * width,
    )
    back = lax.all_to_all(made.reshape(2 * experts, 8, width), ("z", "x", "c"), 0, 0, tiled=True)

    return call(
        combine_kernel,
        out_shape=jax.ShapeDtypeStruct((rows, width), BF),
        in_specs=[VM, VM, VM],
        out_specs=VM,
        compiler_params=pltpu.CompilerParams(vmem_limit_bytes=8 << 20),
        name="combine",
    )(picks, shares, back.reshape(experts * cap, width))


def solution(mesh):
    split = Mesh(mesh.devices.reshape(12, 4, 8, 2), ("z", "x", "y", "c"))
    ep, tp = ("z", "x"), ("y", "c")
    in_specs = (
        P(ep, tp),
        P(tp),
        P(ep, None),
        P(ep, None),
        P(ep, None, tp),
        P(ep, None, tp),
        P(ep, None, tp),
    )
    return jax.shard_map(body, mesh=split, in_specs=in_specs, out_specs=P(ep, tp), check_vma=False)
```

```python
import functools

import jax
import jax.numpy as jnp
from jax import lax
from jax.experimental import pallas as pl
from jax.experimental.pallas import tpu as pltpu
from jax.sharding import Mesh, PartitionSpec as P

BF = jnp.bfloat16
F32 = jnp.float32
VM = pl.BlockSpec(memory_space=pltpu.VMEM)
STEPS = (0, 1, -1, 2, -2, 3, -3, 4)
PAD = 8


def dot(a, b):
    return jnp.dot(a, b, preferred_element_type=F32)


def dispatch_kernel(experts, cap, ids_ref, tok_ref, out_ref, pick_ref):
    rows = tok_ref.shape[0]
    expert = lax.broadcasted_iota(jnp.int32, (experts, rows), 0)
    named = (expert == ids_ref[0:1, :]) | (expert == ids_ref[1:2, :])
    before = lax.broadcasted_iota(jnp.int32, (rows, rows), 0) < lax.broadcasted_iota(
        jnp.int32, (rows, rows), 1
    )
    rank = dot(named.astype(F32).astype(BF), before.astype(F32).astype(BF))
    rank = jnp.where(named, rank, -1.0)
    slot = lax.broadcasted_iota(jnp.int32, (cap, rows), 0).astype(F32)
    for e in range(experts):
        pick_ref[e * cap : (e + 1) * cap, :] = (
            (rank[e : e + 1, :] == slot).astype(F32).astype(BF)
        )
    out_ref[...] = dot(pick_ref[...], tok_ref[...]).astype(BF)


def plan_kernel(experts, cap, ids_ref, weight_ref, pick_ref, share_ref):
    rows = pick_ref.shape[1]
    line = lax.broadcasted_iota(jnp.int32, (8, rows), 0)
    table = jnp.where(line == 0, ids_ref[0:1, :].astype(F32), 0.0)
    table = jnp.where(line == 1, ids_ref[1:2, :].astype(F32), table)
    table = jnp.where(line == 2, weight_ref[0:1, :], table)
    table = jnp.where(line == 3, weight_ref[1:2, :], table)
    column = table.T
    first, second = column[:, 0:1], column[:, 1:2]
    lanes = lax.broadcasted_iota(jnp.int32, (rows, 128), 1).astype(F32)
    named = (lanes == first) | (lanes == second)
    after = lax.broadcasted_iota(jnp.int32, (rows, rows), 1) < lax.broadcasted_iota(
        jnp.int32, (rows, rows), 0
    )
    rank = dot(after.astype(F32).astype(BF), named.astype(F32).astype(BF))
    place = lax.broadcasted_iota(jnp.int32, (rows, experts * cap), 1).astype(F32)
    for k, name in enumerate((first, second)):
        mine = jnp.sum(jnp.where(lanes == name, rank, 0.0), axis=1, keepdims=True)
        pick_ref[k] = (place == name * cap + mine).astype(F32).astype(BF)
        share_ref[k] = jnp.broadcast_to(column[:, 2 + k : 3 + k], (rows, 128))


def combine_kernel(pick_ref, share_ref, back_ref, out_ref):
    total = None
    for k in range(2):
        term = dot(pick_ref[k], back_ref[...]) * share_ref[k][:, :1]
        total = term if k == 0 else total + term
    out_ref[...] = total.astype(BF)


def pack_kernel(came_ref, gain_ref, out_ref):
    sources = came_ref.shape[0] // 2
    width = came_ref.shape[2]
    for s in range(sources):
        for c in range(2):
            out_ref[s * 8 : s * 8 + 8, c * width : (c + 1) * width] = came_ref[2 * s + c]
    gain = jnp.concatenate([gain_ref[0], gain_ref[1]], axis=1)
    top = gain.astype(BF).astype(F32)
    mid = (gain - top).astype(BF).astype(F32)
    low = gain - top - mid
    line = lax.broadcasted_iota(jnp.int32, (PAD, 2 * width), 0)
    split = jnp.where(line == 0, top, jnp.where(line == 1, mid, jnp.where(line == 2, low, 0.0)))
    out_ref[sources * 8 : sources * 8 + PAD, :] = split.astype(BF)


def source_of(step, count):
    turn = 1 - 2 * lax.axis_index("c")
    return lax.rem(lax.axis_index("y") - step * turn + 2 * count, count)


def take(refs, sizes):
    parts, at = [], 0
    for size in sizes:
        parts.append(refs[at : at + size])
        at += size
    return parts


def hidden_kernel(count, skip, inputs, last, *refs):
    kept = 3 if skip else 0
    blocks, weights, before, outs = take(refs, (inputs, 4, kept, len(refs) - inputs - 4 - kept))
    gate_ref, gate2_ref, up_ref, up2_ref = weights
    depth = blocks[0].shape[1]
    rows, half = blocks[0].shape[0] - PAD, gate_ref.shape[1]
    total = [ref[...] for ref in before] if skip else None
    for step, block in zip(STEPS[skip : skip + inputs], blocks):
        start = pl.multiple_of(source_of(step, count) * depth, depth)
        gain = jnp.sum(block[rows : rows + PAD, :].astype(F32), axis=0, keepdims=True)
        raw = block[0:rows, :].astype(F32)
        squares = raw * raw
        part = squares[:, 0:128]
        for lane in range(128, depth, 128):
            part = part + squares[:, lane : lane + 128]
        scaled = (raw * gain).astype(BF)
        gate = jnp.concatenate([gate_ref[pl.ds(start, depth), :], gate2_ref[pl.ds(start, depth), :]], axis=1)
        up = jnp.concatenate([up_ref[pl.ds(start, depth), :], up2_ref[pl.ds(start, depth), :]], axis=1)
        new = [dot(scaled, gate), dot(scaled, up), part]
        total = new if total is None else [t + n for t, n in zip(total, new)]
    if not last:
        for ref, value in zip(outs, total):
            ref[...] = value
        return
    mean = jnp.sum(total[2], axis=1, keepdims=True) / (depth * count)
    scale = lax.rsqrt(mean + 1e-06)
    gate, up = total[0] * scale, total[1] * scale
    hidden = (gate / (1.0 + jnp.exp(-gate)) * up).astype(BF)
    core = lax.axis_index("c")
    outs[0][:, pl.ds(pl.multiple_of(core * half, half), half)] = hidden[:, :half]
    outs[0][:, pl.ds(pl.multiple_of((1 - core) * half, half), half)] = hidden[:, half:]


def down_kernel(count, skip, inputs, last, *refs):
    kept = 2 if skip else 0
    blocks, weights, before, outs = take(refs, (inputs, 2, kept, len(refs) - inputs - 2 - kept))
    rows, depth = blocks[0].shape
    total = [ref[...] for ref in before] if skip else None
    for step, block in zip(STEPS[skip : skip + inputs], blocks):
        start = pl.multiple_of(source_of(step, count) * depth, depth)
        new = [dot(block[...], ref[pl.ds(start, depth), :]) for ref in weights]
        total = new if total is None else [t + n for t, n in zip(total, new)]
    if not last:
        for ref, value in zip(outs, total):
            ref[...] = value
        return
    core = lax.axis_index("c")
    for s in range(rows // 8):
        outs[0][s, core] = total[0][s * 8 : s * 8 + 8, :].astype(BF)
        outs[0][s, 1 - core] = total[1][s * 8 : s * 8 + 8, :].astype(BF)


def ring(block, count):
    def perm(sign):
        return [
            (y * 2 + c, (y + sign * (1 - 2 * c)) % count * 2 + c) for y in range(count) for c in range(2)
        ]

    main = other = block
    found = [block]
    for k in range(3):
        main = lax.ppermute(main, ("y", "c"), perm(1))
        other = lax.ppermute(other, ("y", "c"), perm(-1))
        found += [main, other]
    found.append(lax.ppermute(main, ("y", "c"), perm(1)))
    return found


def swap(value):
    return lax.ppermute(value, "c", [(0, 1), (1, 0)])


def body(tokens, norm_gain, expert_ids, expert_weights, gate_weight, up_weight, down_weight):
    count = lax.axis_size("y")
    experts = lax.axis_size("z") * lax.axis_size("x")
    rows, width = tokens.shape
    cap = 3 * rows * expert_ids.shape[1] // (2 * experts)
    half = experts * cap // 2
    ids = expert_ids.T
    call = pl.pallas_call

    outgoing = call(
        functools.partial(dispatch_kernel, experts, cap),
        out_shape=jax.ShapeDtypeStruct((experts * cap, width), BF),
        in_specs=[VM, VM],
        out_specs=VM,
        scratch_shapes=[pltpu.VMEM((experts * cap, rows), BF)],
        name="dispatch",
    )(ids, tokens)
    came = lax.all_to_all(outgoing.reshape(2 * experts, 8, width), ("z", "x", "c"), 0, 0, tiled=True)

    picks, shares = call(
        functools.partial(plan_kernel, experts, cap),
        out_shape=[
            jax.ShapeDtypeStruct((2, rows, experts * cap), BF),
            jax.ShapeDtypeStruct((2, rows, 128), F32),
        ],
        in_specs=[VM, VM],
        out_specs=[VM, VM],
        compiler_params=pltpu.CompilerParams(vmem_limit_bytes=8 << 20),
        cost_estimate=pl.CostEstimate(flops=1 << 30, bytes_accessed=1 << 20, transcendentals=0),
        name="plan",
    )(ids, expert_weights.T)
    gate, up, down = gate_weight[0], up_weight[0], down_weight[0]
    came, gains, picks, shares = lax.optimization_barrier(
        (came, lax.all_gather(norm_gain[None], "c", axis=0), picks, shares)
    )
    gate2, up2, down2 = swap(gate), swap(up), swap(down)
    block = call(
        pack_kernel,
        out_shape=jax.ShapeDtypeStruct((half + PAD, 2 * width), BF),
        in_specs=[VM, VM],
        out_specs=VM,
        compiler_params=pltpu.CompilerParams(vmem_limit_bytes=8 << 20),
        name="pack",
    )(came, gains)

    def product(kernel, name, found, weights, sums, outs, each):
        total, skip = [], 0
        for group in (found,):
            last = skip + len(group) == count
            shapes = outs if last else sums
            total = call(
                functools.partial(kernel, count, skip, len(group), last),
                out_shape=shapes,
                in_specs=[VM] * (len(group) + len(weights) + len(total)),
                out_specs=[VM] * len(shapes),
                compiler_params=pltpu.CompilerParams(vmem_limit_bytes=16 << 20),
                cost_estimate=pl.CostEstimate(
                    flops=len(group) * each, bytes_accessed=1 << 20, transcendentals=0
                ),
                name=name,
            )(*group, *weights, *total)
            skip += len(group)
        return total

    ff = gate.shape[1]
    (hidden,) = product(
        hidden_kernel,
        "hidden",
        ring(block, count),
        (gate, gate2, up, up2),
        [jax.ShapeDtypeStruct((half, 2 * ff), F32)] * 2 + [jax.ShapeDtypeStruct((half, 128), F32)],
        [jax.ShapeDtypeStruct((half, 2 * ff), BF)],
        2 * half * 2 * width * 4 * ff,
    )
    (made,) = product(
        down_kernel,
        "down",
        ring(hidden, count),
        (down, down2),
        [jax.ShapeDtypeStruct((half, width), F32)] * 2,
        [jax.ShapeDtypeStruct((experts, 2, 8, width), BF)],
        2 * half * 2 * ff * 2 * width,
    )
    back = lax.all_to_all(made.reshape(2 * experts, 8, width), ("z", "x", "c"), 0, 0, tiled=True)

    return call(
        combine_kernel,
        out_shape=jax.ShapeDtypeStruct((rows, width), BF),
        in_specs=[VM, VM, VM],
        out_specs=VM,
        compiler_params=pltpu.CompilerParams(vmem_limit_bytes=8 << 20),
        name="combine",
    )(picks, shares, back.reshape(experts * cap, width))


def solution(mesh):
    split = Mesh(mesh.devices.reshape(12, 4, 8, 2), ("z", "x", "y", "c"))
    ep, tp = ("z", "x"), ("y", "c")
    in_specs = (
        P(ep, tp),
        P(tp),
        P(ep, None),
        P(ep, None),
        P(ep, None, tp),
        P(ep, None, tp),
        P(ep, None, tp),
    )
    return jax.shard_map(body, mesh=split, in_specs=in_specs, out_specs=P(ep, tp), check_vma=False)
```

```python
import functools

import jax
import jax.numpy as jnp
from jax import lax
from jax.experimental import pallas as pl
from jax.experimental.pallas import tpu as pltpu
from jax.sharding import Mesh, PartitionSpec as P

BF = jnp.bfloat16
F32 = jnp.float32
VM = pl.BlockSpec(memory_space=pltpu.VMEM)
STEPS = (0, 1, -1, 2, -2, 3, -3, 4)
PAD = 8


def dot(a, b):
    return jnp.dot(a, b, preferred_element_type=F32)


def dispatch_kernel(experts, cap, ids_ref, tok_ref, out_ref, pick_ref):
    rows = tok_ref.shape[0]
    expert = lax.broadcasted_iota(jnp.int32, (experts, rows), 0)
    named = (expert == ids_ref[0:1, :]) | (expert == ids_ref[1:2, :])
    before = lax.broadcasted_iota(jnp.int32, (rows, rows), 0) < lax.broadcasted_iota(
        jnp.int32, (rows, rows), 1
    )
    rank = dot(named.astype(F32).astype(BF), before.astype(F32).astype(BF))
    rank = jnp.where(named, rank, -1.0)
    slot = lax.broadcasted_iota(jnp.int32, (cap, rows), 0).astype(F32)
    for e in range(experts):
        pick_ref[e * cap : (e + 1) * cap, :] = (
            (rank[e : e + 1, :] == slot).astype(F32).astype(BF)
        )
    out_ref[...] = dot(pick_ref[...], tok_ref[...]).astype(BF)


def plan_kernel(experts, cap, ids_ref, weight_ref, pick_ref, share_ref):
    rows = pick_ref.shape[1]
    line = lax.broadcasted_iota(jnp.int32, (8, rows), 0)
    table = jnp.where(line == 0, ids_ref[0:1, :].astype(F32), 0.0)
    table = jnp.where(line == 1, ids_ref[1:2, :].astype(F32), table)
    table = jnp.where(line == 2, weight_ref[0:1, :], table)
    table = jnp.where(line == 3, weight_ref[1:2, :], table)
    column = table.T
    first, second = column[:, 0:1], column[:, 1:2]
    lanes = lax.broadcasted_iota(jnp.int32, (rows, 128), 1).astype(F32)
    named = (lanes == first) | (lanes == second)
    after = lax.broadcasted_iota(jnp.int32, (rows, rows), 1) < lax.broadcasted_iota(
        jnp.int32, (rows, rows), 0
    )
    rank = dot(after.astype(F32).astype(BF), named.astype(F32).astype(BF))
    place = lax.broadcasted_iota(jnp.int32, (rows, experts * cap), 1).astype(F32)
    for k, name in enumerate((first, second)):
        mine = jnp.sum(jnp.where(lanes == name, rank, 0.0), axis=1, keepdims=True)
        pick_ref[k] = (place == name * cap + mine).astype(F32).astype(BF)
        share_ref[k] = jnp.broadcast_to(column[:, 2 + k : 3 + k], (rows, 128))


def combine_kernel(pick_ref, share_ref, back_ref, out_ref):
    total = None
    for k in range(2):
        term = dot(pick_ref[k], back_ref[...]) * share_ref[k][:, :1]
        total = term if k == 0 else total + term
    out_ref[...] = total.astype(BF)


def pack_kernel(came_ref, gain_ref, out_ref):
    sources = came_ref.shape[0] // 2
    width = came_ref.shape[2]
    for s in range(sources):
        for c in range(2):
            out_ref[s * 8 : s * 8 + 8, c * width : (c + 1) * width] = came_ref[2 * s + c]
    gain = jnp.concatenate([gain_ref[0], gain_ref[1]], axis=1)
    top = gain.astype(BF).astype(F32)
    mid = (gain - top).astype(BF).astype(F32)
    low = gain - top - mid
    line = lax.broadcasted_iota(jnp.int32, (PAD, 2 * width), 0)
    split = jnp.where(line == 0, top, jnp.where(line == 1, mid, jnp.where(line == 2, low, 0.0)))
    out_ref[sources * 8 : sources * 8 + PAD, :] = split.astype(BF)


def source_of(step, count):
    turn = 1 - 2 * lax.axis_index("c")
    return lax.rem(lax.axis_index("y") - step * turn + 2 * count, count)


def partner(y, odd, count):
    return (((y + odd) ^ 1) - odd + count) % count


def exchange_origins(count):
    here, core = lax.axis_index("y"), lax.axis_index("c")

    def path(turns):
        y = here
        for turn in turns:
            odd = core if turn == 0 else 1 - core
            y = lax.rem(((y + odd) ^ 1) - odd + count, count)
        return y

    turns = ((), (0,), (1,), (1, 0), (0, 1), (0, 1, 0), (1, 0, 1), (1, 0, 1, 0))
    return [path(t) for t in turns]


def take(refs, sizes):
    parts, at = [], 0
    for size in sizes:
        parts.append(refs[at : at + size])
        at += size
    return parts


def hidden_kernel(count, skip, inputs, last, *refs):
    kept = 3 if skip else 0
    blocks, weights, before, outs = take(refs, (inputs, 4, kept, len(refs) - inputs - 4 - kept))
    gate_ref, gate2_ref, up_ref, up2_ref = weights
    depth = blocks[0].shape[1]
    rows, half = blocks[0].shape[0] - PAD, gate_ref.shape[1]
    total = [ref[...] for ref in before] if skip else None
    for step, block in zip(STEPS[skip : skip + inputs], blocks):
        start = pl.multiple_of(source_of(step, count) * depth, depth)
        gain = jnp.sum(block[rows : rows + PAD, :].astype(F32), axis=0, keepdims=True)
        raw = block[0:rows, :].astype(F32)
        squares = raw * raw
        part = squares[:, 0:128]
        for lane in range(128, depth, 128):
            part = part + squares[:, lane : lane + 128]
        scaled = (raw * gain).astype(BF)
        gate = jnp.concatenate([gate_ref[pl.ds(start, depth), :], gate2_ref[pl.ds(start, depth), :]], axis=1)
        up = jnp.concatenate([up_ref[pl.ds(start, depth), :], up2_ref[pl.ds(start, depth), :]], axis=1)
        new = [dot(scaled, gate), dot(scaled, up), part]
        total = new if total is None else [t + n for t, n in zip(total, new)]
    if not last:
        for ref, value in zip(outs, total):
            ref[...] = value
        return
    mean = jnp.sum(total[2], axis=1, keepdims=True) / (depth * count)
    scale = lax.rsqrt(mean + 1e-06)
    gate, up = total[0] * scale, total[1] * scale
    hidden = (gate / (1.0 + jnp.exp(-gate)) * up).astype(BF)
    core = lax.axis_index("c")
    outs[0][:, pl.ds(pl.multiple_of(core * half, half), half)] = hidden[:, :half]
    outs[0][:, pl.ds(pl.multiple_of((1 - core) * half, half), half)] = hidden[:, half:]


def down_kernel(count, skip, inputs, last, *refs):
    kept = 2 if skip else 0
    blocks, weights, before, outs = take(refs, (inputs, 2, kept, len(refs) - inputs - 2 - kept))
    rows, depth = blocks[0].shape
    total = [ref[...] for ref in before] if skip else None
    for place, block in zip(exchange_origins(count)[skip : skip + inputs], blocks):
        start = pl.multiple_of(place * depth, depth)
        new = [dot(block[...], ref[pl.ds(start, depth), :]) for ref in weights]
        total = new if total is None else [t + n for t, n in zip(total, new)]
    if not last:
        for ref, value in zip(outs, total):
            ref[...] = value
        return
    core = lax.axis_index("c")
    for s in range(rows // 8):
        outs[0][s, core] = total[0][s * 8 : s * 8 + 8, :].astype(BF)
        outs[0][s, 1 - core] = total[1][s * 8 : s * 8 + 8, :].astype(BF)


def ring(block, count):
    def perm(sign):
        return [
            (y * 2 + c, (y + sign * (1 - 2 * c)) % count * 2 + c) for y in range(count) for c in range(2)
        ]

    main = other = block
    found = [block]
    for k in range(3):
        main = lax.ppermute(main, ("y", "c"), perm(1))
        other = lax.ppermute(other, ("y", "c"), perm(-1))
        found += [main, other]
    found.append(lax.ppermute(main, ("y", "c"), perm(1)))
    return found


def exchange(block, count):
    def perm(turn):
        return [
            (y * 2 + c, partner(y, (turn + c) % 2, count) * 2 + c) for y in range(count) for c in range(2)
        ]

    main = other = block
    found = [block]
    for k in range(3):
        main = lax.ppermute(main, ("y", "c"), perm(k))
        other = lax.ppermute(other, ("y", "c"), perm(k + 1))
        found += [main, other]
    found.append(lax.ppermute(main, ("y", "c"), perm(1)))
    return found


def swap(value):
    return lax.ppermute(value, "c", [(0, 1), (1, 0)])


def body(tokens, norm_gain, expert_ids, expert_weights, gate_weight, up_weight, down_weight):
    count = lax.axis_size("y")
    experts = lax.axis_size("z") * lax.axis_size("x")
    rows, width = tokens.shape
    cap = 3 * rows * expert_ids.shape[1] // (2 * experts)
    half = experts * cap // 2
    ids = expert_ids.T
    call = pl.pallas_call

    outgoing = call(
        functools.partial(dispatch_kernel, experts, cap),
        out_shape=jax.ShapeDtypeStruct((experts * cap, width), BF),
        in_specs=[VM, VM],
        out_specs=VM,
        scratch_shapes=[pltpu.VMEM((experts * cap, rows), BF)],
        name="dispatch",
    )(ids, tokens)
    came = lax.all_to_all(outgoing.reshape(2 * experts, 8, width), ("z", "x", "c"), 0, 0, tiled=True)

    picks, shares = call(
        functools.partial(plan_kernel, experts, cap),
        out_shape=[
            jax.ShapeDtypeStruct((2, rows, experts * cap), BF),
            jax.ShapeDtypeStruct((2, rows, 128), F32),
        ],
        in_specs=[VM, VM],
        out_specs=[VM, VM],
        compiler_params=pltpu.CompilerParams(vmem_limit_bytes=8 << 20),
        cost_estimate=pl.CostEstimate(flops=1 << 30, bytes_accessed=1 << 20, transcendentals=0),
        name="plan",
    )(ids, expert_weights.T)
    gate, up, down = gate_weight[0], up_weight[0], down_weight[0]
    came, gains, picks, shares = lax.optimization_barrier(
        (came, lax.all_gather(norm_gain[None], "c", axis=0), picks, shares)
    )
    gate2, up2, down2 = swap(gate), swap(up), swap(down)
    block = call(
        pack_kernel,
        out_shape=jax.ShapeDtypeStruct((half + PAD, 2 * width), BF),
        in_specs=[VM, VM],
        out_specs=VM,
        compiler_params=pltpu.CompilerParams(vmem_limit_bytes=8 << 20),
        name="pack",
    )(came, gains)

    def product(kernel, name, found, weights, sums, outs, each):
        total, skip = [], 0
        for group in (found,):
            last = skip + len(group) == count
            shapes = outs if last else sums
            total = call(
                functools.partial(kernel, count, skip, len(group), last),
                out_shape=shapes,
                in_specs=[VM] * (len(group) + len(weights) + len(total)),
                out_specs=[VM] * len(shapes),
                compiler_params=pltpu.CompilerParams(vmem_limit_bytes=16 << 20),
                cost_estimate=pl.CostEstimate(
                    flops=len(group) * each, bytes_accessed=1 << 20, transcendentals=0
                ),
                name=name,
            )(*group, *weights, *total)
            skip += len(group)
        return total

    ff = gate.shape[1]
    (hidden,) = product(
        hidden_kernel,
        "hidden",
        ring(block, count),
        (gate, gate2, up, up2),
        [jax.ShapeDtypeStruct((half, 2 * ff), F32)] * 2 + [jax.ShapeDtypeStruct((half, 128), F32)],
        [jax.ShapeDtypeStruct((half, 2 * ff), BF)],
        2 * half * 2 * width * 4 * ff,
    )
    (made,) = product(
        down_kernel,
        "down",
        exchange(hidden, count),
        (down, down2),
        [jax.ShapeDtypeStruct((half, width), F32)] * 2,
        [jax.ShapeDtypeStruct((experts, 2, 8, width), BF)],
        2 * half * 2 * ff * 2 * width,
    )
    back = lax.all_to_all(made.reshape(2 * experts, 8, width), ("z", "x", "c"), 0, 0, tiled=True)

    return call(
        combine_kernel,
        out_shape=jax.ShapeDtypeStruct((rows, width), BF),
        in_specs=[VM, VM, VM],
        out_specs=VM,
        compiler_params=pltpu.CompilerParams(vmem_limit_bytes=8 << 20),
        name="combine",
    )(picks, shares, back.reshape(experts * cap, width))


def solution(mesh):
    split = Mesh(mesh.devices.reshape(12, 4, 8, 2), ("z", "x", "y", "c"))
    ep, tp = ("z", "x"), ("y", "c")
    in_specs = (
        P(ep, tp),
        P(tp),
        P(ep, None),
        P(ep, None),
        P(ep, None, tp),
        P(ep, None, tp),
        P(ep, None, tp),
    )
    return jax.shard_map(body, mesh=split, in_specs=in_specs, out_specs=P(ep, tp), check_vma=False)
```

```python
import functools

import jax
import jax.numpy as jnp
from jax import lax
from jax.experimental import pallas as pl
from jax.experimental.pallas import tpu as pltpu
from jax.sharding import Mesh, PartitionSpec as P


BF = jnp.bfloat16
F32 = jnp.float32
VM = pl.BlockSpec(memory_space=pltpu.VMEM)
STEPS = (0, 1, -1, 2, -2, 3, -3, 4)
PAD = 8


def dot(a, b):
    return jnp.dot(a, b, preferred_element_type=F32)


def dispatch_kernel(experts, cap, ids_ref, tok_ref, out_ref, pick_ref):
    rows = tok_ref.shape[0]
    expert = lax.broadcasted_iota(jnp.int32, (experts, rows), 0)
    named = (expert == ids_ref[0:1, :]) | (expert == ids_ref[1:2, :])
    before = lax.broadcasted_iota(jnp.int32, (rows, rows), 0) < lax.broadcasted_iota(
        jnp.int32, (rows, rows), 1
    )
    rank = dot(named.astype(F32).astype(BF), before.astype(F32).astype(BF))
    rank = jnp.where(named, rank, -1.0)
    slot = lax.broadcasted_iota(jnp.int32, (cap, rows), 0).astype(F32)
    for e in range(experts):
        pick_ref[e * cap : (e + 1) * cap, :] = (
            (rank[e : e + 1, :] == slot).astype(F32).astype(BF)
        )
    out_ref[...] = dot(pick_ref[...], tok_ref[...]).astype(BF)


def plan_kernel(experts, cap, ids_ref, weight_ref, pick_ref, share_ref):
    rows = pick_ref.shape[1]
    line = lax.broadcasted_iota(jnp.int32, (8, rows), 0)
    table = jnp.where(line == 0, ids_ref[0:1, :].astype(F32), 0.0)
    table = jnp.where(line == 1, ids_ref[1:2, :].astype(F32), table)
    table = jnp.where(line == 2, weight_ref[0:1, :], table)
    table = jnp.where(line == 3, weight_ref[1:2, :], table)
    column = table.T
    first, second = column[:, 0:1], column[:, 1:2]
    lanes = lax.broadcasted_iota(jnp.int32, (rows, 128), 1).astype(F32)
    named = (lanes == first) | (lanes == second)
    after = lax.broadcasted_iota(jnp.int32, (rows, rows), 1) < lax.broadcasted_iota(
        jnp.int32, (rows, rows), 0
    )
    rank = dot(after.astype(F32).astype(BF), named.astype(F32).astype(BF))
    place = lax.broadcasted_iota(jnp.int32, (rows, experts * cap), 1).astype(F32)
    for k, name in enumerate((first, second)):
        mine = jnp.sum(jnp.where(lanes == name, rank, 0.0), axis=1, keepdims=True)
        pick_ref[k] = (place == name * cap + mine).astype(F32).astype(BF)
        share_ref[k] = jnp.broadcast_to(column[:, 2 + k : 3 + k], (rows, 128))


def combine_kernel(pick_ref, share_ref, back_ref, out_ref):
    total = None
    for k in range(2):
        term = dot(pick_ref[k], back_ref[...]) * share_ref[k][:, :1]
        total = term if k == 0 else total + term
    out_ref[...] = total.astype(BF)


def pack_kernel(came_ref, gain_ref, out_ref):
    sources = came_ref.shape[0] // 2
    width = came_ref.shape[2]
    for s in range(sources):
        for c in range(2):
            out_ref[s * 8 : s * 8 + 8, c * width : (c + 1) * width] = came_ref[2 * s + c]
    gain = jnp.concatenate([gain_ref[0], gain_ref[1]], axis=1)
    top = gain.astype(BF).astype(F32)
    mid = (gain - top).astype(BF).astype(F32)
    low = gain - top - mid
    line = lax.broadcasted_iota(jnp.int32, (PAD, 2 * width), 0)
    split = jnp.where(line == 0, top, jnp.where(line == 1, mid, jnp.where(line == 2, low, 0.0)))
    out_ref[sources * 8 : sources * 8 + PAD, :] = split.astype(BF)


def source_of(step, count):
    turn = 1 - 2 * lax.axis_index("c")
    return lax.rem(lax.axis_index("y") - step * turn + 2 * count, count)


def take(refs, sizes):
    parts, at = [], 0
    for size in sizes:
        parts.append(refs[at : at + size])
        at += size
    return parts


def hidden_kernel(count, skip, inputs, last, *refs):
    kept = 3 if skip else 0
    blocks, weights, before, outs = take(refs, (inputs, 4, kept, len(refs) - inputs - 4 - kept))
    gate_ref, gate2_ref, up_ref, up2_ref = weights
    depth = blocks[0].shape[1]
    rows, half = blocks[0].shape[0] - PAD, gate_ref.shape[1]
    total = [ref[...] for ref in before] if skip else None
    for step, block in zip(STEPS[skip : skip + inputs], blocks):
        start = pl.multiple_of(source_of(step, count) * depth, depth)
        gain = jnp.sum(block[rows : rows + PAD, :].astype(F32), axis=0, keepdims=True)
        raw = block[0:rows, :].astype(F32)
        squares = raw * raw
        part = squares[:, 0:128]
        for lane in range(128, depth, 128):
            part = part + squares[:, lane : lane + 128]
        scaled = (raw * gain).astype(BF)
        gate = jnp.concatenate([gate_ref[pl.ds(start, depth), :], gate2_ref[pl.ds(start, depth), :]], axis=1)
        up = jnp.concatenate([up_ref[pl.ds(start, depth), :], up2_ref[pl.ds(start, depth), :]], axis=1)
        new = [dot(scaled, gate), dot(scaled, up), part]
        total = new if total is None else [t + n for t, n in zip(total, new)]
    if not last:
        for ref, value in zip(outs, total):
            ref[...] = value
        return
    mean = jnp.sum(total[2], axis=1, keepdims=True) / (depth * count)
    scale = lax.rsqrt(mean + 1e-06)
    gate, up = total[0] * scale, total[1] * scale
    hidden = (gate / (1.0 + jnp.exp(-gate)) * up).astype(BF)
    core = lax.axis_index("c")
    outs[0][:, pl.ds(pl.multiple_of(core * half, half), half)] = hidden[:, :half]
    outs[0][:, pl.ds(pl.multiple_of((1 - core) * half, half), half)] = hidden[:, half:]


def down_kernel(count, skip, inputs, last, *refs):
    kept = 2 if skip else 0
    blocks, weights, before, outs = take(refs, (inputs, 2, kept, len(refs) - inputs - 2 - kept))
    rows, depth = blocks[0].shape
    total = [ref[...] for ref in before] if skip else None
    for step, block in zip(STEPS[skip : skip + inputs], blocks):
        start = pl.multiple_of(source_of(step, count) * depth, depth)
        new = [dot(block[...], ref[pl.ds(start, depth), :]) for ref in weights]
        total = new if total is None else [t + n for t, n in zip(total, new)]
    if not last:
        for ref, value in zip(outs, total):
            ref[...] = value
        return
    core = lax.axis_index("c")
    for s in range(rows // 8):
        outs[0][s, core] = total[0][s * 8 : s * 8 + 8, :].astype(BF)
        outs[0][s, 1 - core] = total[1][s * 8 : s * 8 + 8, :].astype(BF)


def ring(block, count):
    def perm(sign):
        return [
            (y * 2 + c, (y + sign * (1 - 2 * c)) % count * 2 + c) for y in range(count) for c in range(2)
        ]

    main = other = block
    found = [block]
    for _ in range(3):
        main = lax.ppermute(main, ("y", "c"), perm(1))
        other = lax.ppermute(other, ("y", "c"), perm(-1))
        found += [main, other]
    found.append(lax.ppermute(main, ("y", "c"), perm(1)))
    return found


def swap(value):
    return lax.ppermute(value, "c", [(0, 1), (1, 0)])


def layer(tokens, norm_gain, expert_ids, expert_weights, gate_weight, up_weight, down_weight):
    count = lax.axis_size("y")
    experts = lax.axis_size("z") * lax.axis_size("x")
    rows, width = tokens.shape
    cap = 3 * rows * expert_ids.shape[1] // (2 * experts)
    half = experts * cap // 2
    ids = expert_ids.T
    call = pl.pallas_call

    outgoing = call(
        functools.partial(dispatch_kernel, experts, cap),
        out_shape=jax.ShapeDtypeStruct((experts * cap, width), BF),
        in_specs=[VM, VM],
        out_specs=VM,
        scratch_shapes=[pltpu.VMEM((experts * cap, rows), BF)],
        name="dispatch",
    )(ids, tokens)
    came = lax.all_to_all(outgoing.reshape(2 * experts, 8, width), ("z", "x", "c"), 0, 0, tiled=True)

    picks, shares = call(
        functools.partial(plan_kernel, experts, cap),
        out_shape=[
            jax.ShapeDtypeStruct((2, rows, experts * cap), BF),
            jax.ShapeDtypeStruct((2, rows, 128), F32),
        ],
        in_specs=[VM, VM],
        out_specs=[VM, VM],
        compiler_params=pltpu.CompilerParams(vmem_limit_bytes=8 << 20),
        cost_estimate=pl.CostEstimate(flops=1 << 30, bytes_accessed=1 << 20, transcendentals=0),
        name="plan",
    )(ids, expert_weights.T)
    gate, up, down = gate_weight[0], up_weight[0], down_weight[0]
    came, gains, picks, shares = lax.optimization_barrier(
        (came, lax.all_gather(norm_gain[None], "c", axis=0), picks, shares)
    )
    gate2 = swap(gate)
    up2 = swap(up)
    down2 = swap(down)
    block = call(
        pack_kernel,
        out_shape=jax.ShapeDtypeStruct((half + PAD, 2 * width), BF),
        in_specs=[VM, VM],
        out_specs=VM,
        compiler_params=pltpu.CompilerParams(vmem_limit_bytes=8 << 20),
        name="pack",
    )(came, gains)

    def product(kernel, found, weights, sums, outs, each):
        total, skip = [], 0
        for group in (found,):
            last = skip + len(group) == count
            shapes = outs if last else sums
            total = call(
                functools.partial(kernel, count, skip, len(group), last),
                out_shape=shapes,
                in_specs=[VM] * (len(group) + len(weights) + len(total)),
                out_specs=[VM] * len(shapes),
                compiler_params=pltpu.CompilerParams(vmem_limit_bytes=16 << 20),
                cost_estimate=pl.CostEstimate(
                    flops=len(group) * each, bytes_accessed=1 << 20, transcendentals=0
                ),
            )(*group, *weights, *total)
            skip += len(group)
        return total

    ff = gate.shape[1]
    (hidden,) = product(
        hidden_kernel,
        ring(block, count),
        (gate, gate2, up, up2),
        [jax.ShapeDtypeStruct((half, 2 * ff), F32)] * 2 + [jax.ShapeDtypeStruct((half, 128), F32)],
        [jax.ShapeDtypeStruct((half, 2 * ff), BF)],
        2 * half * 2 * width * 4 * ff,
    )
    (made,) = product(
        down_kernel,
        ring(hidden, count),
        (down, down2),
        [jax.ShapeDtypeStruct((half, width), F32)] * 2,
        [jax.ShapeDtypeStruct((experts, 2, 8, width), BF)],
        2 * half * 2 * ff * 2 * width,
    )
    back = lax.all_to_all(made.reshape(2 * experts, 8, width), ("z", "x", "c"), 0, 0, tiled=True)

    return call(
        combine_kernel,
        out_shape=jax.ShapeDtypeStruct((rows, width), BF),
        in_specs=[VM, VM, VM],
        out_specs=VM,
        compiler_params=pltpu.CompilerParams(vmem_limit_bytes=8 << 20),
        name="combine",
    )(picks, shares, back.reshape(experts * cap, width))


def solution(mesh):
    split = Mesh(mesh.devices.reshape(12, 4, 8, 2), ("z", "x", "y", "c"))
    ep, tp = ("z", "x"), ("y", "c")
    in_specs = (
        P(ep, tp),
        P(tp),
        P(ep, None),
        P(ep, None),
        P(ep, None, tp),
        P(ep, None, tp),
        P(ep, None, tp),
    )
    return jax.shard_map(layer, mesh=split, in_specs=in_specs, out_specs=P(ep, tp), check_vma=False)
```
